512 devices in a mesh: sp: 32 (over z, core), tp: 16 (over y, x).
Axes of the slice: x: 4, y: 4, z: 16, core: 2. Of those that a mesh axis runs over, the one named last changes fastest.
Arguments:
- queries: bfloat16 [8192, 2048], P('sp', 'tp'), may hold values from -6 to 6
- keys: bfloat16 [8192, 256], P('sp'), may hold values from -6 to 6
- values: bfloat16 [8192, 256], P('sp'), may hold values from -6 to 6
- query_gain: float32 [128], replicated, may hold values from 0.1 to 5.5
- key_gain: float32 [128], replicated, may hold values from 0.1 to 5.5
- out_proj: bfloat16 [2048, 2048], P(None, 'tp'), may hold values from -0.125 to 0.125
- expert_norm_scale: float32 [2048], replicated, may hold values from 0.1 to 1.9
- residual: bfloat16 [8192, 2048], P(('sp', 'tp')), may hold values from -6 to 6
- routes: int32 [8192, 2], P(('sp', 'tp')), may hold values from 0 to 31, all different within a row; in each aligned block of 16 rows (0 to 15, 16 to 31, ...) at most 2 rows name the same one
- route_weights: float32 [8192, 2], P(('sp', 'tp')), may hold values from 0.1 to 0.9
- w_gate: bfloat16 [32, 2048, 4096], P('sp', None, 'tp'), may hold values from -0.125 to 0.125
- w_up: bfloat16 [32, 2048, 4096], P('sp', None, 'tp'), may hold values from -0.125 to 0.125
- w_down: bfloat16 [32, 4096, 2048], P('sp', 'tp'), may hold values from -0.09375 to 0.09375
Outputs:
- layer_out: bfloat16 [8192, 2048], P(('sp', 'tp'))
The draws below stay inside these ranges and needn't reach their ends.
Inputs may be any that keep to these rules, and one draw needn't show every extreme that they name: `routes`: in the rows of one device no expert is named by more than 2 rows, a bound that some block reaches; a row names 2 different experts.
All inputs are finite; a program needn't handle non-finite values.
Results may differ from the reference program's by a relative error of at most 0.0095.
The reference program's roundings to bfloat16 on the way count: a program that leaves them out, or rounds other values in their place, can miss the bound.
Values may be sent and summed in bfloat16 or wider, within the bound.
No kernel may reach another device: no remote copies, remote signals or barrier semaphores. Data moves between devices by JAX's collectives and lax.ppermute only.
A program may use at most 64 MiB of HBM per device.

```python
import math
import jax
import jax.numpy as jnp
import numpy as np
from jax import lax

D = 2048
HD = 128
HEADS = 16
KV = 2
FF = 4096
TOP = 2
GRID_W = 64
TOKENS = 8192
TOK_DEV = 16
EXPERTS = 32
CAP = 2
N_TP = 16


def shared_keys(key):
    base = jax.random.normal(jax.random.fold_in(key, 101), (TOKENS, KV * HD), jnp.float32)
    return jnp.clip(base, -6.0, 6.0)


def draw_keys(key, part):
    return shared_keys(key).astype(jnp.bfloat16)


def draw_queries(key, part):
    base = jax.random.normal(jax.random.fold_in(key, 202), (TOKENS, HEADS * HD), jnp.float32)
    base = jnp.clip(base, -6.0, 6.0)
    return base.astype(jnp.bfloat16)


def draw_query_gain(key, part):
    uniform_draw = jax.random.uniform(jax.random.fold_in(key, 303), (HD,), jnp.float32)
    return 0.1 + 1.8 * uniform_draw


def draw_key_gain(key, part):
    uniform_draw = jax.random.uniform(jax.random.fold_in(key, 404), (HD,), jnp.float32)
    return 0.1 + 1.8 * uniform_draw


def shard_levels(stream_key, dims, pieces, smallest, largest):
    def one(dim, blocks):
        heights = jax.random.uniform(jax.random.fold_in(jax.random.fold_in(stream_key, 6), dim), (blocks,), jnp.float32, smallest / len(pieces), largest / len(pieces))
        return jnp.repeat(jnp.exp(heights), dims[dim] // blocks).reshape((-1,) + (1,) * (len(dims) - dim - 1))

    level = one(*pieces[0])
    for cut in pieces[1:]:
        level = level * one(*cut)
    return level


def assign_block(own_key, own, number, rows, count, top, bound, skew):
    ranking = jax.random.permutation(own_key, count)
    packed, common = load_shares(count, rows * top, bound, skew, True), load_shares(count, rows * top, bound, skew, False)
    places = jnp.arange(count)

    def named(lengths, offset_by):
        used = int((lengths > 0).sum())
        fixed = max(1, used // 4)
        shifted = fixed + (places - fixed + offset_by * (used - fixed)) % max(1, count - fixed)
        return jnp.zeros((count,), jnp.int32).at[ranking[jnp.where(places < fixed, places, shifted)]].set(jnp.asarray(lengths, jnp.int32))

    lengths = jnp.where(number % 4 == 0, named(packed, number // 4), named(common, number - number // 4 - 1))
    mixed = jax.random.permutation(jax.random.fold_in(own, 3), count)
    source_of, taker = mixed[0:count // 2 * 2:2], mixed[1:count // 2 * 2:2]
    slack = jnp.minimum(lengths[source_of] - 1, bound - lengths[taker]) // 2
    slack = jnp.where((source_of == ranking[0]) | (taker == ranking[0]) | (lengths[taker] == 0), 0, jnp.maximum(slack, 0))
    shifted = jax.random.randint(jax.random.fold_in(own, 4), (count // 2,), 0, 1 << 20) % (slack + 1)
    lengths = lengths.at[source_of].add(-shifted).at[taker].add(shifted)
    labels = jnp.searchsorted(jnp.cumsum(lengths), jnp.arange(rows * top), side="right").astype(jnp.int32)
    grid = labels.reshape(top, rows).T
    grid = grid[jax.random.permutation(jax.random.fold_in(own, 1), rows)]
    offset_by = jax.random.randint(jax.random.fold_in(own, 2), (rows, 1), 0, top)
    return jnp.take_along_axis(grid, (jnp.arange(top)[None, :] + offset_by) % top, axis=1)


def load_shares(number_of, total, most, skew, full):
    weights = [(1 << 20) // math.isqrt(rank ** skew) + 1 for rank in range(1, number_of + 1)]
    largest = most if full else min(most, max(-(-total // number_of), total * weights[0] // sum(weights)))
    least = 1 if total - largest >= number_of - 1 else 0
    holding, rest = [largest] + [least] * (number_of - 1), total - largest - least * (number_of - 1)
    while rest > 0:
        candidates = [i for i in range(1, number_of) if holding[i] < largest] or [i for i in range(1, number_of) if holding[i] < most]
        mass, remaining = sum([weights[i] for i in candidates]), rest
        for i in candidates:
            extra = min(most - holding[i], max(1, remaining * weights[i] // mass), rest)
            holding[i] = holding[i] + extra
            rest = rest - extra
    return np.array(holding)


def centred(key, extent, scale, reach, split=(), held_as=jnp.bfloat16):
    result = scale * jax.random.normal(key, extent, jnp.float32)
    if split:
        result = result * shard_levels(key, extent, split, -0.22, 0.18)
    return jnp.clip(result, -reach, reach).astype(held_as)


def setup_inputs(seed: int = 0) -> dict:
    streams_of = jax.random.split(jax.random.key(seed), 14)
    queries = draw_queries(jax.random.fold_in(streams_of[13], 71), 0)
    keys = draw_keys(jax.random.fold_in(streams_of[13], 71), 0)
    values = centred(streams_of[2], (TOKENS, KV * HD), 1.0, 6.0, ((0, 32),))
    query_gain = draw_query_gain(jax.random.fold_in(streams_of[13], 71), 0)
    key_gain = draw_key_gain(jax.random.fold_in(streams_of[13], 71), 0)
    out_proj = centred(streams_of[5], (HEADS * HD, D), (HEADS * HD) ** -0.5, 0.125, ((1, 16),))
    expert_norm_scale = jnp.clip(1.0 + 0.18 * jax.random.normal(streams_of[6], (D,), jnp.float32), 0.1, 1.9)
    residual = centred(streams_of[7], (TOKENS, D), 1.0, 6.0, ((0, 512),))
    routes_keys = jax.random.split(jax.random.fold_in(streams_of[8], 1), TOKENS // TOK_DEV)
    routes_turns = jax.random.permutation(jax.random.fold_in(streams_of[8], 3), TOKENS // TOK_DEV)
    routes = jax.vmap(lambda own, number: assign_block(jax.random.fold_in(streams_of[8], 2), own, number, TOK_DEV, EXPERTS, TOP, CAP, 1))(routes_keys, routes_turns).reshape((TOKENS, TOP))
    route_weights = jnp.clip(0.1 + 0.79999997 * jax.random.uniform(streams_of[9], (TOKENS, TOP), jnp.float32) ** shard_levels(streams_of[9], (TOKENS, TOP), ((0, 512),), -0.2, 0.2), 0.1, 0.9)
    w_gate = centred(streams_of[10], (EXPERTS, D, FF), D ** -0.5, 0.125, ((0, 32), (2, 16)))
    w_up = centred(streams_of[11], (EXPERTS, D, FF), D ** -0.5, 0.125, ((0, 32), (2, 16)))
    w_down = centred(streams_of[12], (EXPERTS, FF, D), FF ** -0.5, 0.09375, ((0, 32), (1, 16)))
    return dict(queries=queries, keys=keys, values=values, query_gain=query_gain, key_gain=key_gain, out_proj=out_proj, expert_norm_scale=expert_norm_scale, residual=residual, routes=routes, route_weights=route_weights, w_gate=w_gate, w_up=w_up, w_down=w_down)


EPS = 1e-06
ROPE_BASE = 10000.0

def rotate(field, position):
    half = field.shape[-1] // 2
    quarter = half // 2
    freqs = ROPE_BASE ** (-jnp.arange(quarter, dtype=jnp.float32) / quarter)
    grid_row = (position // GRID_W).astype(jnp.float32)
    grid_col = (position % GRID_W).astype(jnp.float32)

    def turn_half(part, coord):
        angle = coord[:, None] * freqs[None, :]
        cosine = jnp.cos(angle)[:, None, :]
        sine = jnp.sin(angle)[:, None, :]
        first, second = (part[..., :quarter], part[..., quarter:])
        return jnp.concatenate([first * cosine - second * sine, second * cosine + first * sine], axis=-1)
    return jnp.concatenate([turn_half(field[..., :half], grid_row), turn_half(field[..., half:], grid_col)], axis=-1)

def prepare(field, gain, position):
    count = field.shape[0]
    width = gain.shape[0]
    heads_here = field.shape[1] // width
    values_f = field.reshape(count, heads_here, width).astype(jnp.float32)
    scaled = values_f * lax.rsqrt(lax.optimization_barrier(jnp.mean(values_f * values_f, axis=-1, keepdims=True)) + EPS) * gain
    return rotate(scaled, position).reshape(count, heads_here * width).astype(jnp.bfloat16)

def reference(queries, keys, values, query_gain, key_gain, out_proj, expert_norm_scale, residual, routes, route_weights, w_gate, w_up, w_down):
    position = jnp.arange(TOKENS, dtype=jnp.int32)
    q_rot = prepare(queries, query_gain, position)
    k_rot = prepare(keys, key_gain, position)
    group = HEADS // KV
    block = math.gcd(TOKENS, 1024)

    def one_head(head):
        shared_value_head = head // group
        query_cols = lax.dynamic_slice_in_dim(q_rot, (head * HD).astype(jnp.int32), HD, 1)
        key_cols = lax.dynamic_slice_in_dim(k_rot, (shared_value_head * HD).astype(jnp.int32), HD, 1)
        value_cols = lax.dynamic_slice_in_dim(values, (shared_value_head * HD).astype(jnp.int32), HD, 1)

        def attend(query_block):
            scores = jnp.dot(query_block, key_cols.T, preferred_element_type=jnp.float32) * HD ** (-0.5)
            row_max = lax.optimization_barrier(jnp.max(scores, axis=-1, keepdims=True))
            weight_tensors = jnp.exp(scores - row_max).astype(jnp.bfloat16)
            total = lax.optimization_barrier(jnp.sum(lax.optimization_barrier(weight_tensors).astype(jnp.float32), axis=-1, keepdims=True))
            summed = jnp.dot(weight_tensors, value_cols, preferred_element_type=jnp.float32)
            return (summed / total).astype(jnp.bfloat16)
        blocks = query_cols.reshape(TOKENS // block, block, HD)
        return lax.map(attend, blocks).reshape(TOKENS, HD)
    per_head = lax.map(one_head, jnp.arange(HEADS, dtype=jnp.int32))
    attn = per_head.transpose(1, 0, 2).reshape(TOKENS, HEADS * HD)
    projected = jnp.dot(attn, out_proj, preferred_element_type=jnp.float32).astype(jnp.bfloat16)
    mixed = (residual.astype(jnp.float32) + projected.astype(jnp.float32)).astype(jnp.bfloat16)
    mixed_float_output = mixed.astype(jnp.float32)
    normed = (mixed_float_output * lax.rsqrt(lax.optimization_barrier(jnp.mean(mixed_float_output * mixed_float_output, axis=-1, keepdims=True)) + EPS) * expert_norm_scale).astype(jnp.bfloat16)
    flat_routes = routes.reshape(-1)
    flat_weights = route_weights.reshape(-1)
    flat_token = jnp.arange(TOKENS * TOP, dtype=jnp.int32) // TOP
    most_rows = TOKENS // TOK_DEV * CAP
    block_ff = FF // N_TP

    def expert_step(totals, expert):
        order = jnp.argsort((flat_routes != expert).astype(jnp.int32), stable=True)[:most_rows].astype(jnp.int32)
        valid = flat_routes[order] == expert
        rows = normed[flat_token[order]]
        gate = jnp.dot(rows, w_gate[expert], preferred_element_type=jnp.float32)
        upper = jnp.dot(rows, w_up[expert], preferred_element_type=jnp.float32)
        hidden = (jax.nn.silu(gate) * upper).astype(jnp.bfloat16)
        hidden_blocks = hidden.reshape(most_rows, N_TP, block_ff).astype(jnp.float32)
        down_blocks = w_down[expert].reshape(N_TP, block_ff, D).astype(jnp.float32)
        partial_value = jnp.einsum('mjf,jfd->jmd', hidden_blocks, down_blocks).astype(jnp.bfloat16)
        summed = lax.optimization_barrier(jnp.sum(lax.optimization_barrier(partial_value).astype(jnp.float32), axis=0))
        expert_out = summed.astype(jnp.bfloat16)
        weighted = lax.optimization_barrier(expert_out).astype(jnp.float32) * flat_weights[order][:, None]
        weighted = jnp.where(valid[:, None], weighted, jnp.float32(0.0))
        return (totals.at[order].add(weighted), None)
    start = jnp.zeros((TOKENS * TOP, D), jnp.float32)
    totals, unused = lax.scan(expert_step, start, jnp.arange(EXPERTS, dtype=jnp.int32))
    moe_sum = lax.optimization_barrier(jnp.sum(totals.reshape(TOKENS, TOP, D), axis=1))
    return (mixed_float_output + moe_sum).astype(jnp.bfloat16)
```

```python
import jax
import jax.numpy as jnp
from jax import lax
from jax.experimental import pallas as pl
from jax.experimental.pallas import tpu as pltpu
from jax.sharding import Mesh, PartitionSpec as P

GRID_W = 64
EPS = 1e-06
ROPE_BASE = 10000.0
LOG2E = 1.4426950408889634
BF = jnp.bfloat16
F32 = jnp.float32

NZ, NC, NYH, NYL, NX = 16, 2, 2, 2, 4
NY = NYH * NYL
NT = NY * NX
NG = NYL * NX
TP = ("yh", "yl", "x")
GROUP = ("yl", "x")
STAT_ROWS = 16


def spread(value, axis, count):
    copies = jnp.broadcast_to(value, (count, *value.shape))
    return lax.all_to_all(copies, axis, split_axis=0, concat_axis=0, tiled=True)


def swap_cores(value):
    return lax.ppermute(value, "c", [(0, 1), (1, 0)])


def ring(value, axis, step):
    return lax.ppermute(value, axis, [(i, (i + step) % 4) for i in range(4)])


def prepare(field, gain, position):
    width = field.shape[1]
    half, quarter = width // 2, width // 4
    freqs = ROPE_BASE ** (-jnp.arange(quarter, dtype=F32) / quarter)
    grid_row = (position // GRID_W).astype(F32)
    grid_col = (position % GRID_W).astype(F32)
    f = field.astype(F32)
    f = f * lax.rsqrt(jnp.mean(f * f, axis=-1, keepdims=True) + EPS) * gain

    def turn_half(part, coord):
        angle = coord[:, None] * freqs[None, :]
        cosine, sine = jnp.cos(angle), jnp.sin(angle)
        first, second = part[:, :quarter], part[:, quarter:]
        return [first * cosine - second * sine, second * cosine + first * sine]

    parts = turn_half(f[:, :half], grid_row) + turn_half(f[:, half:], grid_col)
    return jnp.concatenate(parts, axis=-1).astype(BF)


def split3(x):
    hi = x.astype(BF)
    rest = x - hi.astype(F32)
    mid = rest.astype(BF)
    lo = (rest - mid.astype(F32)).astype(BF)
    return hi, mid, lo


def attend_kernel(q_ref, own_ref, other_ref, out_ref):
    width = q_ref.shape[2]
    factor = width ** (-0.5) * LOG2E
    keys = jnp.concatenate([own_ref[:, :width], other_ref[:, :width]], axis=0)
    values = jnp.concatenate([own_ref[:, width:], other_ref[:, width:]], axis=0)
    scores = lax.dot_general(
        keys, q_ref[0], (((1,), (1,)), ((), ())), preferred_element_type=F32
    )
    top = jnp.max(scores, axis=0, keepdims=True)
    weights = jnp.exp2((scores - top) * factor).astype(BF)
    total = jnp.sum(weights.astype(F32), axis=0, keepdims=True)
    summed = lax.dot_general(
        values, weights, (((0,), (0,)), ((), ())), preferred_element_type=F32
    )
    out_ref[0, :width, :] = (summed / total).astype(BF)
    cols = summed.shape[1]
    row = lax.broadcasted_iota(jnp.int32, (STAT_ROWS, cols), 0)
    stats = jnp.zeros((STAT_ROWS, cols), F32)
    for i, part in enumerate(split3(top * factor) + split3(total)):
        stats = jnp.where(row == i, part.astype(F32), stats)
    out_ref[0, width:, :] = stats.astype(BF)


def attend(q8, own, other):
    heads, rows, width = q8.shape
    return pl.pallas_call(
        attend_kernel,
        grid=(heads,),
        in_specs=[
            pl.BlockSpec((1, rows, width), lambda h: (h, 0, 0)),
            pl.BlockSpec(own.shape, lambda h: (0, 0)),
            pl.BlockSpec(other.shape, lambda h: (0, 0)),
        ],
        out_specs=pl.BlockSpec((1, width + STAT_ROWS, rows), lambda h: (h, 0, 0)),
        out_shape=jax.ShapeDtypeStruct((heads, width + STAT_ROWS, rows), BF),
        name="attend",
    )(q8, own, other)


def combine_kernel(parts_ref, out_ref):
    count = parts_ref.shape[0]
    width = out_ref.shape[0]
    tops, totals = [], []
    for j in range(count):
        s = parts_ref[j, width:, :].astype(F32)
        tops.append(s[0:1] + s[1:2] + s[2:3])
        totals.append(s[3:4] + s[4:5] + s[5:6])
    top = tops[0]
    for j in range(1, count):
        top = jnp.maximum(top, tops[j])
    shares = [totals[j] * jnp.exp2(tops[j] - top) for j in range(count)]
    whole = sum(shares[1:], shares[0])
    acc = jnp.zeros(out_ref.shape, F32)
    for j in range(count):
        acc = acc + parts_ref[j, :width, :].astype(F32) * (shares[j] / whole)
    out_ref[...] = acc.astype(BF)


def combine(parts):
    width = parts.shape[1] - STAT_ROWS
    return pl.pallas_call(
        combine_kernel,
        out_shape=jax.ShapeDtypeStruct((width, parts.shape[2]), BF),
        name="combine",
    )(parts)


def experts_kernel(rows_ref, *refs):
    pieces, out_ref, held, acc, sems = refs[:-4], refs[-4], refs[-3], refs[-2], refs[-1]
    count, depth, _ = held.shape
    copies, waits = [], [[] for _ in range(count)]
    chunk, at = 0, 0
    for i, piece in enumerate(pieces):
        size = piece.shape[0]
        copy = pltpu.make_async_copy(piece, held.at[chunk, pl.ds(at, size), :], sems.at[i])
        copy.start()
        waits[chunk].append(copy)
        at += size
        if at == depth:
            chunk, at = chunk + 1, 0
    units = held.shape[2] // 3
    for pair in range(count // 2):
        hidden, down = [], []
        for k in (2 * pair, 2 * pair + 1):
            for copy in waits[k]:
                copy.wait()
            both = jnp.dot(
                rows_ref[...], held[k, :, : 2 * units], preferred_element_type=F32
            )
            gate, upper = both[:, :units], both[:, units:]
            hidden.append((gate / (1.0 + jnp.exp(-gate)) * upper).astype(BF))
            down.append(held[k, :, 2 * units :])
        part = lax.dot_general(
            jnp.concatenate(hidden, axis=1),
            jnp.concatenate(down, axis=1),
            (((1,), (1,)), ((), ())),
            preferred_element_type=F32,
        )
        if pair == 0:
            acc[...] = part
        elif pair < count // 2 - 1:
            acc[...] += part
        else:
            out_ref[...] = (acc[...] + part).astype(BF)


def experts(rows, pieces):
    depth = sum(p.shape[0] for p in pieces) // 8
    width = pieces[0].shape[1]
    return pl.pallas_call(
        experts_kernel,
        in_specs=[pl.BlockSpec(memory_space=pltpu.VMEM)]
        + [pl.BlockSpec(memory_space=pl.ANY)] * len(pieces),
        out_specs=pl.BlockSpec(memory_space=pltpu.VMEM),
        out_shape=jax.ShapeDtypeStruct(rows.shape, BF),
        scratch_shapes=[
            pltpu.VMEM((8, depth, width), BF),
            pltpu.VMEM(rows.shape, F32),
            pltpu.SemaphoreType.DMA((len(pieces),)),
        ],
        compiler_params=pltpu.CompilerParams(vmem_limit_bytes=40 * 1024 * 1024),
        name="experts",
    )(rows, *pieces)


def local(
    queries,
    keys,
    values,
    query_gain,
    key_gain,
    out_proj,
    expert_norm_scale,
    residual,
    routes,
    route_weights,
    w_gate,
    w_up,
    w_down,
):
    width = query_gain.shape[0]
    tok_sp = queries.shape[0]
    tok_dev, depth = residual.shape
    top = routes.shape[1]
    z, c = lax.axis_index("z"), lax.axis_index("c")
    yh, yl, x = lax.axis_index("yh"), lax.axis_index("yl"), lax.axis_index("x")
    start = (z * NC + c) * tok_sp

    slice_len = tok_sp // NG
    at = (yl * NX + x) * slice_len
    own_key = lax.dynamic_slice(keys, (at, yh * width), (slice_len, width))
    own_value = lax.dynamic_slice(values, (at, yh * width), (slice_len, width))
    key_pos = start + at + jnp.arange(slice_len, dtype=jnp.int32)
    own_kv = jnp.concatenate([prepare(own_key, key_gain, key_pos), own_value], axis=1)
    kv_mine = spread(own_kv, "z", NZ).reshape(NZ * slice_len, 2 * width)
    kv_other = swap_cores(kv_mine)

    q_rot = prepare(queries, query_gain, start + jnp.arange(tok_sp, dtype=jnp.int32))
    q8 = spread(q_rot, GROUP, NG)

    units = w_gate.shape[2] // 2
    packs = [
        jnp.concatenate(
            [w_gate[0][:, s], w_up[0][:, s], w_down[0][s, :].T], axis=1
        )
        for s in (slice(0, units), slice(units, 2 * units))
    ]
    pieces = []
    for pack, axis in zip(packs, ("x", ("yh", "yl"))):
        left, right = ring(pack, axis, 1), ring(pack, axis, -1)
        upper = ring(left[: depth // 2], axis, 1)
        lower = ring(right[depth // 2 :], axis, -1)
        pieces += [pack, left, right, upper, lower]

    parts = attend(q8, kv_mine, kv_other)
    parts = lax.all_to_all(parts, GROUP, split_axis=0, concat_axis=0, tiled=True)
    attn = combine(parts)
    attn_all = spread(attn, TP, NT).reshape(NT * width, tok_sp)
    columns = lax.dot_general(
        attn_all, out_proj, (((0,), (0,)), ((), ())), preferred_element_type=F32
    ).astype(BF)
    projected = lax.all_to_all(columns, TP, split_axis=0, concat_axis=1, tiled=True)
    mixed = (residual.astype(F32) + projected.astype(F32)).astype(BF)
    mixed_f = mixed.astype(F32)
    normed = (
        mixed_f
        * lax.rsqrt(jnp.mean(mixed_f * mixed_f, axis=-1, keepdims=True) + EPS)
        * expert_norm_scale
    ).astype(BF)

    cap = max(2, 2 * tok_dev * top // (NZ * NC))
    tok = jnp.arange(tok_dev, dtype=jnp.int32)
    before = tok[None, :] < tok[:, None]
    place = jnp.arange(NZ * NC * cap, dtype=jnp.int32)
    rel, zc_slot = place // (NZ * cap), place % (NZ * cap)
    expert_of = (zc_slot // cap) * NC + (c + rel) % NC
    slot_of = zc_slot % cap
    hits = []
    for k in range(top):
        mine = routes[:, k]
        slot = sum(
            jnp.sum(
                ((mine[:, None] == routes[:, j][None, :]) & before).astype(jnp.int32), axis=1
            )
            for j in range(top)
        )
        hits.append(
            (mine[:, None] == expert_of[None, :]) & (slot[:, None] == slot_of[None, :])
        )
    selector = sum(h.astype(BF) for h in hits)
    sent = lax.dot_general(
        selector, normed, (((0,), (0,)), ((), ())), preferred_element_type=F32
    ).astype(BF)
    half = NZ * cap
    from_other = swap_cores(sent[half:])
    outgoing = jnp.concatenate(
        [sent[:half].reshape(NZ, cap, depth), from_other.reshape(NZ, cap, depth)], axis=1
    )
    arrived = lax.all_to_all(outgoing, "z", split_axis=0, concat_axis=0, tiled=True)

    by_class = arrived.reshape(4, NZ * NC * cap // 4, depth)
    order = [(i % NX + i // NX) % 4 for i in range(NT)]
    to_send = jnp.stack([by_class[k] for k in order])
    rows = lax.all_to_all(to_send, TP, split_axis=0, concat_axis=0, tiled=True)
    partial = experts(rows.reshape(-1, depth), pieces).reshape(rows.shape)
    back = lax.all_to_all(partial, TP, split_axis=0, concat_axis=0, tiled=True)
    expert_out = jnp.stack(
        [
            sum(back[i].astype(F32) for i in range(NT) if order[i] == k).astype(BF)
            for k in range(4)
        ]
    ).reshape(NZ, NC * cap, depth)
    returned = lax.all_to_all(expert_out, "z", split_axis=0, concat_axis=0, tiled=True)
    for_other = swap_cores(returned[:, cap:].reshape(half, depth))
    picked_from = jnp.concatenate([returned[:, :cap].reshape(half, depth), for_other], axis=0)
    moe = sum(
        jnp.dot(hits[k].astype(BF), picked_from, preferred_element_type=F32)
        * route_weights[:, k][:, None]
        for k in range(top)
    )
    return (mixed_f + moe).astype(BF)


def solution(mesh):
    fine = Mesh(
        mesh.devices.reshape(NZ, NC, NYH, NYL, NX), ("z", "c", "yh", "yl", "x")
    )
    sp, both = ("z", "c"), ("z", "c", "yh", "yl", "x")
    placed = (
        P(sp, TP),
        P(sp, None),
        P(sp, None),
        P(),
        P(),
        P(None, TP),
        P(),
        P(both, None),
        P(both, None),
        P(both, None),
        P(sp, None, TP),
        P(sp, None, TP),
        P(sp, TP, None),
    )
    return jax.shard_map(
        local, mesh=fine, in_specs=placed, out_specs=P(both, None), check_vma=False
    )
```

```python
import math

import jax
import jax.numpy as jnp
from jax import lax
from jax.experimental import pallas as pl
from jax.experimental.pallas import tpu as pltpu
from jax.sharding import Mesh, PartitionSpec as P


GRID_W = 64
EPS = 1e-06
ROPE_BASE = 10000.0
LOG2E = 1.4426950408889634
BF = jnp.bfloat16
F32 = jnp.float32

NZ, NC, NYH, NYL, NX = 16, 2, 2, 2, 4
NY = NYH * NYL
NT = NY * NX
NG = NYL * NX
TP = ("yh", "yl", "x")
GROUP = ("yl", "x")
STAT_ROWS = 16
COLOURS = tuple((i % NX + i // NX) % 4 for i in range(NT))


def exchange(blocks, axis):
    return lax.all_to_all(blocks, axis, split_axis=0, concat_axis=0, tiled=True)


def swap_cores(value):
    return lax.ppermute(value, "c", [(0, 1), (1, 0)])


def ring(value, axis, step):
    return lax.ppermute(value, axis, [(i, (i + step) % 4) for i in range(4)])


def turned(field, gain, start):
    count, width = field.shape
    quarter = width // 4
    f = field.astype(F32)
    f = f * lax.rsqrt(jnp.mean(f * f, axis=-1, keepdims=True) + EPS) * gain
    lane = lax.broadcasted_iota(jnp.int32, (count, width), 1)
    position = start + lax.broadcasted_iota(jnp.int32, (count, width), 0)
    coord = jnp.where(lane < 2 * quarter, position // GRID_W, position % GRID_W)
    step = (lane % quarter).astype(F32) / quarter
    angle = coord.astype(F32) * jnp.exp(step * (-math.log(ROPE_BASE)))
    first = lane % (2 * quarter) < quarter
    ahead = pltpu.roll(f, width - quarter, 1)
    behind = pltpu.roll(f, quarter, 1)
    other = jnp.where(first, -ahead, behind)
    return (f * jnp.cos(angle) + other * jnp.sin(angle)).astype(BF)


def prepare_kernel(at_ref, q_ref, k_ref, v_ref, q_gain_ref, k_gain_ref, q8_ref, kv_ref):
    q_rot = turned(q_ref[...], q_gain_ref[...], at_ref[2])
    for i in range(q8_ref.shape[0]):
        q8_ref[i] = q_rot
    k_rot = turned(k_ref[...], k_gain_ref[...], at_ref[3])
    both = jnp.concatenate([k_rot, v_ref[...]], axis=1)
    for i in range(kv_ref.shape[0]):
        kv_ref[i] = both


def prepare(queries, keys, values, query_gain, key_gain, block, head, start):
    tokens, width = queries.shape
    size = tokens // NG
    at = jnp.stack([block, head, start, start + block * size]).astype(jnp.int32)
    whole = lambda shape: pl.BlockSpec(shape, lambda i, at: (0,) * len(shape))
    part = pl.BlockSpec((size, width), lambda i, at: (at[0], at[1]))
    outs = ((NG, tokens, width), (NZ, size, 2 * width))
    return pl.pallas_call(
        prepare_kernel,
        grid_spec=pltpu.PrefetchScalarGridSpec(
            num_scalar_prefetch=1,
            grid=(1,),
            in_specs=[whole((tokens, width)), part, part, whole((1, width)), whole((1, width))],
            out_specs=[whole(shape) for shape in outs],
        ),
        out_shape=[jax.ShapeDtypeStruct(shape, BF) for shape in outs],
        name="prepare",
    )(at, queries, keys, values, query_gain[None, :], key_gain[None, :])


def split3(x):
    hi = x.astype(BF)
    rest = x - hi.astype(F32)
    mid = rest.astype(BF)
    lo = (rest - mid.astype(F32)).astype(BF)
    return hi, mid, lo


def attend_kernel(q_ref, own_ref, other_ref, out_ref):
    width = q_ref.shape[2]
    factor = width ** (-0.5) * LOG2E
    keys = jnp.concatenate([own_ref[:, :width], other_ref[:, :width]], axis=0)
    values = jnp.concatenate([own_ref[:, width:], other_ref[:, width:]], axis=0)
    scores = lax.dot_general(
        keys, q_ref[0], (((1,), (1,)), ((), ())), preferred_element_type=F32
    )
    top = jnp.max(scores, axis=0, keepdims=True)
    weights = jnp.exp2((scores - top) * factor).astype(BF)
    total = jnp.sum(weights.astype(F32), axis=0, keepdims=True)
    summed = lax.dot_general(
        values, weights, (((0,), (0,)), ((), ())), preferred_element_type=F32
    )
    out_ref[0, :width, :] = (summed / total).astype(BF)
    cols = summed.shape[1]
    row = lax.broadcasted_iota(jnp.int32, (STAT_ROWS, cols), 0)
    stats = jnp.zeros((STAT_ROWS, cols), F32)
    for i, part in enumerate(split3(top * factor) + split3(total)):
        stats = jnp.where(row == i, part.astype(F32), stats)
    out_ref[0, width:, :] = stats.astype(BF)


def attend(q8, own, other):
    heads, rows, width = q8.shape
    return pl.pallas_call(
        attend_kernel,
        grid=(heads,),
        in_specs=[
            pl.BlockSpec((1, rows, width), lambda h: (h, 0, 0)),
            pl.BlockSpec(own.shape, lambda h: (0, 0)),
            pl.BlockSpec(other.shape, lambda h: (0, 0)),
        ],
        out_specs=pl.BlockSpec((1, width + STAT_ROWS, rows), lambda h: (h, 0, 0)),
        out_shape=jax.ShapeDtypeStruct((heads, width + STAT_ROWS, rows), BF),
        name="attend",
    )(q8, own, other)


def combine_kernel(parts_ref, out_ref):
    count = parts_ref.shape[0]
    width = out_ref.shape[1]
    tops, totals = [], []
    for j in range(count):
        s = parts_ref[j, width:, :].astype(F32)
        tops.append(s[0:1] + s[1:2] + s[2:3])
        totals.append(s[3:4] + s[4:5] + s[5:6])
    top = tops[0]
    for j in range(1, count):
        top = jnp.maximum(top, tops[j])
    shares = [totals[j] * jnp.exp2(tops[j] - top) for j in range(count)]
    whole = sum(shares[1:], shares[0])
    acc = jnp.zeros(out_ref.shape[1:], F32)
    for j in range(count):
        acc = acc + parts_ref[j, :width, :].astype(F32) * (shares[j] / whole)
    done = acc.astype(BF)
    for i in range(out_ref.shape[0]):
        out_ref[i] = done


def combine(parts):
    width = parts.shape[1] - STAT_ROWS
    return pl.pallas_call(
        combine_kernel,
        out_shape=jax.ShapeDtypeStruct((NT, width, parts.shape[2]), BF),
        name="combine",
    )(parts)


def deal_kernel(classes_ref, out_ref):
    for i, k in enumerate(COLOURS):
        out_ref[i] = classes_ref[k]


def deal(classes):
    return pl.pallas_call(
        deal_kernel,
        out_shape=jax.ShapeDtypeStruct((NT, *classes.shape[1:]), BF),
        name="deal",
    )(classes)


def experts_kernel(rows_ref, *refs):
    pieces, out_ref, held, acc, sems = refs[:-4], refs[-4], refs[-3], refs[-2], refs[-1]
    count, depth, _ = held.shape
    waits = [[] for _ in range(count)]
    chunk, at = 0, 0
    for i, piece in enumerate(pieces):
        size = piece.shape[0]
        copy = pltpu.make_async_copy(piece, held.at[chunk, pl.ds(at, size), :], sems.at[i])
        copy.start()
        waits[chunk].append(copy)
        at += size
        if at == depth:
            chunk, at = chunk + 1, 0
    units = held.shape[2] // 3
    for pair in range(count // 2):
        hidden, down = [], []
        for k in (2 * pair, 2 * pair + 1):
            for copy in waits[k]:
                copy.wait()
            both = jnp.dot(
                rows_ref[...], held[k, :, : 2 * units], preferred_element_type=F32
            )
            gate, upper = both[:, :units], both[:, units:]
            hidden.append((gate / (1.0 + jnp.exp(-gate)) * upper).astype(BF))
            down.append(held[k, :, 2 * units :])
        part = lax.dot_general(
            jnp.concatenate(hidden, axis=1),
            jnp.concatenate(down, axis=1),
            (((1,), (1,)), ((), ())),
            preferred_element_type=F32,
        )
        if pair == 0:
            acc[...] = part
        elif pair < count // 2 - 1:
            acc[...] += part
        else:
            out_ref[...] = (acc[...] + part).astype(BF)


def experts(rows, pieces):
    depth = sum(p.shape[0] for p in pieces) // 8
    width = pieces[0].shape[1]
    return pl.pallas_call(
        experts_kernel,
        in_specs=[pl.BlockSpec(memory_space=pltpu.VMEM)]
        + [pl.BlockSpec(memory_space=pl.ANY)] * len(pieces),
        out_specs=pl.BlockSpec(memory_space=pltpu.VMEM),
        out_shape=jax.ShapeDtypeStruct(rows.shape, BF),
        scratch_shapes=[
            pltpu.VMEM((8, depth, width), BF),
            pltpu.VMEM(rows.shape, F32),
            pltpu.SemaphoreType.DMA((len(pieces),)),
        ],
        compiler_params=pltpu.CompilerParams(vmem_limit_bytes=40 * 1024 * 1024),
        name="experts",
    )(rows, *pieces)


def local(
    queries,
    keys,
    values,
    query_gain,
    key_gain,
    out_proj,
    expert_norm_scale,
    residual,
    routes,
    route_weights,
    w_gate,
    w_up,
    w_down,
):
    width = query_gain.shape[0]
    tok_sp = queries.shape[0]
    tok_dev, depth = residual.shape
    top = routes.shape[1]
    z, c = lax.axis_index("z"), lax.axis_index("c")
    yh, yl, x = lax.axis_index("yh"), lax.axis_index("yl"), lax.axis_index("x")
    start = (z * NC + c) * tok_sp

    q8, kv = prepare(
        queries, keys, values, query_gain, key_gain, yl * NX + x, yh, start
    )
    q8 = exchange(q8, GROUP)
    q8, kv = lax.optimization_barrier((q8, kv))
    kv_mine = exchange(kv, "z").reshape(-1, 2 * width)
    kv_other = swap_cores(kv_mine)

    units = w_gate.shape[2] // 2
    pieces = []
    for s, axis in ((slice(0, units), "x"), (slice(units, 2 * units), ("yh", "yl"))):
        pack = jnp.concatenate([w_gate[0][:, s], w_up[0][:, s], w_down[0][s, :].T], axis=1)
        left, right = ring(pack, axis, 1), ring(pack, axis, -1)
        far = ring(left, axis, 1)
        pieces += [pack, left, right, far]

    parts = attend(q8, kv_mine, kv_other)
    parts = exchange(parts, GROUP)
    attn_all = exchange(combine(parts), TP).reshape(NT * width, tok_sp)
    columns = lax.dot_general(
        attn_all, out_proj, (((0,), (0,)), ((), ())), preferred_element_type=F32
    ).astype(BF)
    projected = lax.all_to_all(columns, TP, split_axis=0, concat_axis=1, tiled=True)
    mixed = (residual.astype(F32) + projected.astype(F32)).astype(BF)
    mixed_f = mixed.astype(F32)
    normed = (
        mixed_f
        * lax.rsqrt(jnp.mean(mixed_f * mixed_f, axis=-1, keepdims=True) + EPS)
        * expert_norm_scale
    ).astype(BF)

    cap = max(2, 2 * tok_dev * top // (NZ * NC))
    tok = jnp.arange(tok_dev, dtype=jnp.int32)
    before = tok[None, :] < tok[:, None]
    place = jnp.arange(NZ * NC * cap, dtype=jnp.int32)
    rel, zc_slot = place // (NZ * cap), place % (NZ * cap)
    expert_of = (zc_slot // cap) * NC + (c + rel) % NC
    slot_of = zc_slot % cap
    hits = []
    for k in range(top):
        mine = routes[:, k]
        slot = sum(
            jnp.sum(
                ((mine[:, None] == routes[:, j][None, :]) & before).astype(jnp.int32), axis=1
            )
            for j in range(top)
        )
        hits.append(
            (mine[:, None] == expert_of[None, :]) & (slot[:, None] == slot_of[None, :])
        )
    selector = sum(h.astype(BF) for h in hits)
    sent = lax.dot_general(
        selector, normed, (((0,), (0,)), ((), ())), preferred_element_type=F32
    ).astype(BF)
    half = NZ * cap
    from_other = swap_cores(sent[half:])
    outgoing = jnp.concatenate(
        [sent[:half].reshape(NZ, cap, depth), from_other.reshape(NZ, cap, depth)], axis=1
    )
    arrived = exchange(outgoing, "z")

    rows = exchange(deal(arrived.reshape(4, NZ * NC * cap // 4, depth)), TP)
    partial = experts(rows.reshape(-1, depth), pieces).reshape(rows.shape)
    back = exchange(partial, TP)
    expert_out = jnp.stack(
        [
            sum(back[i].astype(F32) for i in range(NT) if COLOURS[i] == k).astype(BF)
            for k in range(4)
        ]
    ).reshape(NZ, NC * cap, depth)
    returned = exchange(expert_out, "z")
    for_other = swap_cores(returned[:, cap:].reshape(half, depth))
    picked_from = jnp.concatenate([returned[:, :cap].reshape(half, depth), for_other], axis=0)
    moe = sum(
        jnp.dot(hits[k].astype(BF), picked_from, preferred_element_type=F32)
        * route_weights[:, k][:, None]
        for k in range(top)
    )
    return (mixed_f + moe).astype(BF)


def solution(mesh):
    fine = Mesh(
        mesh.devices.reshape(NZ, NC, NYH, NYL, NX), ("z", "c", "yh", "yl", "x")
    )
    sp, both = ("z", "c"), ("z", "c", "yh", "yl", "x")
    placed = (
        P(sp, TP),
        P(sp, None),
        P(sp, None),
        P(),
        P(),
        P(None, TP),
        P(),
        P(both, None),
        P(both, None),
        P(both, None),
        P(sp, None, TP),
        P(sp, None, TP),
        P(sp, TP, None),
    )
    return jax.shard_map(
        local, mesh=fine, in_specs=placed, out_specs=P(both, None), check_vma=False
    )
```

```python
import math

import jax
import jax.numpy as jnp
from jax import lax
from jax.experimental import pallas as pl
from jax.experimental.pallas import tpu as pltpu
from jax.sharding import Mesh, PartitionSpec as P


GRID_W = 64
EPS = 1e-06
ROPE_BASE = 10000.0
LOG2E = 1.4426950408889634
BF = jnp.bfloat16
F32 = jnp.float32

NZ, NC, NYH, NYL, NX = 16, 2, 2, 2, 4
NY = NYH * NYL
NT = NY * NX
NG = NYL * NX
TP = ("yh", "yl", "x")
GROUP = ("yl", "x")
STAT_ROWS = 16
SHARE = 64
COLOURS = tuple((i % NX + i // NX) % 2 for i in range(NT))


IN_VMEM = pl.BlockSpec(memory_space=pltpu.VMEM)
IN_HBM = pl.BlockSpec(memory_space=pltpu.HBM)


def exchange(blocks, axis):
    return lax.all_to_all(blocks, axis, split_axis=0, concat_axis=0, tiled=True)


def swap_cores(value):
    return lax.ppermute(value, "c", [(0, 1), (1, 0)])


def ring(value, axis, step):
    return lax.ppermute(value, axis, [(i, (i + step) % 4) for i in range(4)])


def turned(field, gain, start):
    count, width = field.shape
    quarter = width // 4
    f = field.astype(F32)
    f = f * lax.rsqrt(jnp.mean(f * f, axis=-1, keepdims=True) + EPS) * gain
    lane = lax.broadcasted_iota(jnp.int32, (count, width), 1)
    position = start + lax.broadcasted_iota(jnp.int32, (count, width), 0)
    coord = jnp.where(lane < 2 * quarter, position // GRID_W, position % GRID_W)
    step = (lane % quarter).astype(F32) / quarter
    angle = coord.astype(F32) * jnp.exp(step * (-math.log(ROPE_BASE)))
    first = lane % (2 * quarter) < quarter
    ahead = pltpu.roll(f, width - quarter, 1)
    behind = pltpu.roll(f, quarter, 1)
    other = jnp.where(first, -ahead, behind)
    return (f * jnp.cos(angle) + other * jnp.sin(angle)).astype(BF)


def prepare_kernel(at_ref, q_ref, k_ref, v_ref, q_gain_ref, k_gain_ref, q8_ref, kv_ref):
    q_rot = turned(q_ref[...], q_gain_ref[...], at_ref[2])
    for i in range(q8_ref.shape[0]):
        q8_ref[i] = q_rot
    k_rot = turned(k_ref[...], k_gain_ref[...], at_ref[3])
    both = jnp.concatenate([k_rot, v_ref[...]], axis=1)
    for i in range(kv_ref.shape[0]):
        kv_ref[i] = both


def prepare(queries, keys, values, query_gain, key_gain, block, head, start):
    tokens, width = queries.shape
    size = tokens // NG
    at = jnp.stack([block, head, start, start + block * size]).astype(jnp.int32)
    whole = lambda shape: pl.BlockSpec(shape, lambda i, at: (0,) * len(shape))
    part = pl.BlockSpec((size, width), lambda i, at: (at[0], at[1]))
    outs = ((NG, tokens, width), (NZ, size, 2 * width))
    return pl.pallas_call(
        prepare_kernel,
        grid_spec=pltpu.PrefetchScalarGridSpec(
            num_scalar_prefetch=1,
            grid=(1,),
            in_specs=[whole((tokens, width)), part, part, whole((1, width)), whole((1, width))],
            out_specs=[whole(shape) for shape in outs],
        ),
        out_shape=[jax.ShapeDtypeStruct(shape, BF) for shape in outs],
        name="prepare",
    )(at, queries, keys, values, query_gain[None, :], key_gain[None, :])


def split3(x):
    hi = x.astype(BF)
    rest = x - hi.astype(F32)
    mid = rest.astype(BF)
    lo = (rest - mid.astype(F32)).astype(BF)
    return hi, mid, lo


def attend_kernel(q_ref, own_ref, other_ref, out_ref):
    heads, rows, width = q_ref.shape
    factor = width ** (-0.5) * LOG2E
    keys = jnp.concatenate([own_ref[:, :width], other_ref[:, :width]], axis=0)
    values = jnp.concatenate([own_ref[:, width:], other_ref[:, width:]], axis=0)
    values = jnp.concatenate(
        [values.T, jnp.ones((STAT_ROWS, values.shape[0]), BF)], axis=0
    )
    row = lax.broadcasted_iota(jnp.int32, (STAT_ROWS, rows), 0)
    for head in range(heads):
        scores = lax.dot_general(
            keys, q_ref[head], (((1,), (1,)), ((), ())), preferred_element_type=F32
        )
        top = jnp.max(scores, axis=0, keepdims=True)
        weights = jnp.exp2((scores - top) * factor).astype(BF)
        summed = jnp.dot(values, weights, preferred_element_type=F32)
        total = summed[width : width + 1]
        out_ref[head, :width, :] = (summed[:width] * (1.0 / total)).astype(BF)
        stats = jnp.zeros((STAT_ROWS, rows), F32)
        for i, part in enumerate(split3(top * factor) + split3(total)):
            stats = jnp.where(row == i, part.astype(F32), stats)
        out_ref[head, width:, :] = stats.astype(BF)


def attend(q8, own, other):
    heads, rows, width = q8.shape
    return pl.pallas_call(
        attend_kernel,
        in_specs=[IN_VMEM] * 3,
        out_specs=IN_VMEM,
        out_shape=jax.ShapeDtypeStruct((heads, width + STAT_ROWS, rows), BF),
        name="attend",
    )(q8, own, other)


def combine_kernel(parts_ref, out_ref):
    count = parts_ref.shape[0]
    width = out_ref.shape[1]
    tops, totals = [], []
    for j in range(count):
        s = parts_ref[j, width:, :].astype(F32)
        tops.append(s[0:1] + s[1:2] + s[2:3])
        totals.append(s[3:4] + s[4:5] + s[5:6])
    top = tops[0]
    for j in range(1, count):
        top = jnp.maximum(top, tops[j])
    shares = [totals[j] * jnp.exp2(tops[j] - top) for j in range(count)]
    whole = sum(shares[1:], shares[0])
    acc = jnp.zeros(out_ref.shape[1:], F32)
    for j in range(count):
        acc = acc + parts_ref[j, :width, :].astype(F32) * (shares[j] / whole)
    done = acc.astype(BF)
    for i in range(out_ref.shape[0]):
        out_ref[i] = done


def combine(parts):
    width = parts.shape[1] - STAT_ROWS
    return pl.pallas_call(
        combine_kernel,
        in_specs=[IN_VMEM],
        out_specs=IN_VMEM,
        out_shape=jax.ShapeDtypeStruct((NT, width, parts.shape[2]), BF),
        name="combine",
    )(parts)


def deal_kernel(classes_ref, out_ref):
    for i, k in enumerate(COLOURS):
        out_ref[i] = classes_ref[k]


def deal(classes):
    return pl.pallas_call(
        deal_kernel,
        in_specs=[IN_VMEM],
        out_specs=IN_VMEM,
        out_shape=jax.ShapeDtypeStruct((NT, *classes.shape[1:]), BF),
        name="deal",
    )(classes)


def collect_kernel(back_ref, out_ref):
    for k in range(2):
        total = None
        for i, colour in enumerate(COLOURS):
            if colour == k:
                part = back_ref[i].astype(F32)
                total = part if total is None else total + part
        out_ref[k] = total.astype(BF)


def collect(back):
    return pl.pallas_call(
        collect_kernel,
        in_specs=[IN_VMEM],
        out_specs=IN_VMEM,
        out_shape=jax.ShapeDtypeStruct((2, *back.shape[1:]), BF),
        name="collect",
    )(back)


def pack_kernel(gate_ref, up_ref, down_ref, *out_refs):
    gate, upper, down = gate_ref[0].T, up_ref[0].T, down_ref[0]
    for i in range(2):
        part = slice(i * SHARE, (i + 1) * SHARE)
        packed = jnp.concatenate([gate[part], upper[part], down[part]], axis=0)
        for half in range(2):
            @pl.when(pl.program_id(0) == half)
            def _():
                out_refs[2 * half + i][...] = packed


def pack(w_gate, w_up, w_down):
    _, depth, _ = w_gate.shape
    wide = pl.BlockSpec((1, depth, 2 * SHARE), lambda i: (0, 0, i))
    shape = (3 * SHARE, depth)
    return pl.pallas_call(
        pack_kernel,
        grid=(2,),
        in_specs=[wide, wide, pl.BlockSpec((1, 2 * SHARE, depth), lambda i: (0, i, 0))],
        out_specs=[pl.BlockSpec(shape, lambda i: (0, 0))] * 4,
        out_shape=[jax.ShapeDtypeStruct(shape, BF)] * 4,
        name="pack",
    )(w_gate, w_up, w_down)


def swish(gate, upper):
    return (gate / (1.0 + jnp.exp(-gate)) * upper).astype(BF)


def experts_kernel(rows_ref, gate_hbm, up_hbm, down_hbm, *refs):
    near_hbm, refs = refs[:4], refs[4:]
    out_ref, gate_ref, up_ref, down_ref, near_ref, acc, sems = refs
    jobs = [(gate_hbm.at[0], gate_ref), (up_hbm.at[0], up_ref), (down_hbm.at[0], down_ref)]
    for i, source in enumerate(near_hbm):
        for j in range(3):
            jobs.append(
                (
                    source.at[pl.ds(j * SHARE, SHARE)],
                    near_ref.at[j, pl.ds(i * SHARE, SHARE)],
                )
            )
    copies = [
        pltpu.make_async_copy(source, target, sems.at[i])
        for i, (source, target) in enumerate(jobs)
    ]
    for copy in copies:
        copy.start()
    copies[0].wait()
    gate = jnp.dot(rows_ref[...], gate_ref[...], preferred_element_type=F32)
    copies[1].wait()
    upper = jnp.dot(rows_ref[...], up_ref[...], preferred_element_type=F32)
    hidden = swish(gate, upper)
    copies[2].wait()
    acc[...] = jnp.dot(hidden, down_ref[...], preferred_element_type=F32)
    for copy in copies[3:]:
        copy.wait()
    across = (((1,), (1,)), ((), ()))
    gate = lax.dot_general(rows_ref[...], near_ref[0], across, preferred_element_type=F32)
    upper = lax.dot_general(rows_ref[...], near_ref[1], across, preferred_element_type=F32)
    hidden = swish(gate, upper)
    part = jnp.dot(hidden, near_ref[2], preferred_element_type=F32)
    out_ref[...] = (acc[...] + part).astype(BF)


def experts(rows, w_gate, w_up, w_down, near):
    _, depth, units = w_gate.shape
    return pl.pallas_call(
        experts_kernel,
        in_specs=[IN_VMEM] + [IN_HBM] * (3 + len(near)),
        out_specs=IN_VMEM,
        out_shape=jax.ShapeDtypeStruct(rows.shape, BF),
        scratch_shapes=[
            pltpu.VMEM((depth, units), BF),
            pltpu.VMEM((depth, units), BF),
            pltpu.VMEM((units, depth), BF),
            pltpu.VMEM((3, 4 * SHARE, depth), BF),
            pltpu.VMEM(rows.shape, F32),
            pltpu.SemaphoreType.DMA((3 + 3 * len(near),)),
        ],
        compiler_params=pltpu.CompilerParams(vmem_limit_bytes=40 * 1024 * 1024),
        name="experts",
    )(rows, w_gate, w_up, w_down, *near)


def local(
    queries,
    keys,
    values,
    query_gain,
    key_gain,
    out_proj,
    expert_norm_scale,
    residual,
    routes,
    route_weights,
    w_gate,
    w_up,
    w_down,
):
    width = query_gain.shape[0]
    tok_sp = queries.shape[0]
    tok_dev, depth = residual.shape
    top = routes.shape[1]
    z, c = lax.axis_index("z"), lax.axis_index("c")
    yh, yl, x = lax.axis_index("yh"), lax.axis_index("yl"), lax.axis_index("x")
    start = (z * NC + c) * tok_sp

    q8, kv = prepare(
        queries, keys, values, query_gain, key_gain, yl * NX + x, yh, start
    )
    q8 = exchange(q8, GROUP)
    q8, kv = lax.optimization_barrier((q8, kv))
    kv_mine = exchange(kv, "z").reshape(-1, 2 * width)
    kv_other = swap_cores(kv_mine)

    packs = pack(w_gate, w_up, w_down)
    near = [
        ring(packs[0], "x", 1),
        ring(packs[1], "x", -1),
        ring(packs[2], ("yh", "yl"), 1),
        ring(packs[3], ("yh", "yl"), -1),
    ]

    parts = attend(q8, kv_mine, kv_other)
    parts = exchange(parts, GROUP)
    attn_all = exchange(combine(parts), TP).reshape(NT * width, tok_sp)
    columns = lax.dot_general(
        attn_all, out_proj, (((0,), (0,)), ((), ())), preferred_element_type=F32
    ).astype(BF)
    projected = lax.all_to_all(columns, TP, split_axis=0, concat_axis=1, tiled=True)
    mixed = (residual.astype(F32) + projected.astype(F32)).astype(BF)
    mixed_f = mixed.astype(F32)
    normed = (
        mixed_f
        * lax.rsqrt(jnp.mean(mixed_f * mixed_f, axis=-1, keepdims=True) + EPS)
        * expert_norm_scale
    ).astype(BF)

    cap = max(2, 2 * tok_dev * top // (NZ * NC))
    tok = jnp.arange(tok_dev, dtype=jnp.int32)
    before = tok[None, :] < tok[:, None]
    place = jnp.arange(NZ * NC * cap, dtype=jnp.int32)
    expert_of, slot_of = place // cap, place % cap
    hits = []
    for k in range(top):
        mine = routes[:, k]
        slot = sum(
            jnp.sum(
                ((mine[:, None] == routes[:, j][None, :]) & before).astype(jnp.int32), axis=1
            )
            for j in range(top)
        )
        hits.append(
            (mine[:, None] == expert_of[None, :]) & (slot[:, None] == slot_of[None, :])
        )
    selector = sum(h.astype(BF) for h in hits)
    sent = lax.dot_general(
        selector, normed, (((0,), (0,)), ((), ())), preferred_element_type=F32
    ).astype(BF)
    arrived = exchange(sent, ("z", "c"))

    rows = exchange(deal(arrived.reshape(2, NZ * NC * cap // 2, depth)), TP)
    partial = experts(rows.reshape(-1, depth), w_gate, w_up, w_down, near)
    back = exchange(partial.reshape(rows.shape), TP)
    picked_from = exchange(collect(back).reshape(arrived.shape), ("z", "c"))
    moe = sum(
        jnp.dot(hits[k].astype(BF), picked_from, preferred_element_type=F32)
        * route_weights[:, k][:, None]
        for k in range(top)
    )
    return (mixed_f + moe).astype(BF)


def solution(mesh):
    fine = Mesh(
        mesh.devices.reshape(NZ, NC, NYH, NYL, NX), ("z", "c", "yh", "yl", "x")
    )
    sp, both = ("z", "c"), ("z", "c", "yh", "yl", "x")
    placed = (
        P(sp, TP),
        P(sp, None),
        P(sp, None),
        P(),
        P(),
        P(None, TP),
        P(),
        P(both, None),
        P(both, None),
        P(both, None),
        P(sp, None, TP),
        P(sp, None, TP),
        P(sp, TP, None),
    )
    return jax.shard_map(
        local, mesh=fine, in_specs=placed, out_specs=P(both, None), check_vma=False
    )
```

```python
import math

import jax
import jax.numpy as jnp
from jax import lax
from jax.experimental import pallas as pl
from jax.experimental.pallas import tpu as pltpu
from jax.sharding import Mesh, PartitionSpec as P


GRID_W = 64
EPS = 1e-06
ROPE_BASE = 10000.0
LOG2E = 1.4426950408889634
BF = jnp.bfloat16
F32 = jnp.float32

NZ, NC, NYH, NYL, NX = 16, 2, 2, 2, 4
NY = NYH * NYL
NT = NY * NX
NG = NYL * NX
TP = ("yh", "yl", "x")
GROUP = ("yl", "x")
STAT_ROWS = 16
SHARE = 128
NSHARE = 4
COLOURS = tuple((i % NX + i // NX) % NSHARE for i in range(NT))


IN_VMEM = pl.BlockSpec(memory_space=pltpu.VMEM)
IN_HBM = pl.BlockSpec(memory_space=pltpu.HBM)


def grant(mib):
    return pltpu.CompilerParams(vmem_limit_bytes=mib * 1024 * 1024)


def exchange(blocks, axis):
    return lax.all_to_all(blocks, axis, split_axis=0, concat_axis=0, tiled=True)


def swap_cores(value):
    return lax.ppermute(value, "c", [(0, 1), (1, 0)])


def ring(value, axis, step):
    return lax.ppermute(value, axis, [(i, (i + step) % 4) for i in range(4)])


def turned(field, gain, start):
    count, width = field.shape
    quarter = width // 4
    f = field.astype(F32)
    f = f * lax.rsqrt(jnp.mean(f * f, axis=-1, keepdims=True) + EPS) * gain
    lane = lax.broadcasted_iota(jnp.int32, (count, width), 1)
    position = start + lax.broadcasted_iota(jnp.int32, (count, width), 0)
    coord = jnp.where(lane < 2 * quarter, position // GRID_W, position % GRID_W)
    step = (lane % quarter).astype(F32) / quarter
    angle = coord.astype(F32) * jnp.exp(step * (-math.log(ROPE_BASE)))
    first = lane % (2 * quarter) < quarter
    ahead = pltpu.roll(f, width - quarter, 1)
    behind = pltpu.roll(f, quarter, 1)
    other = jnp.where(first, -ahead, behind)
    return (f * jnp.cos(angle) + other * jnp.sin(angle)).astype(BF)


def prepare_kernel(at_ref, q_ref, k_ref, v_ref, q_gain_ref, k_gain_ref, q8_ref, kv_ref):
    q_rot = turned(q_ref[...], q_gain_ref[...], at_ref[2])
    for i in range(q8_ref.shape[0]):
        q8_ref[i] = q_rot
    k_rot = turned(k_ref[...], k_gain_ref[...], at_ref[3])
    both = jnp.concatenate([k_rot, v_ref[...]], axis=1)
    for i in range(kv_ref.shape[0]):
        kv_ref[i] = both


def prepare(queries, keys, values, query_gain, key_gain, block, head, start):
    tokens, width = queries.shape
    size = tokens // NG
    at = jnp.stack([block, head, start, start + block * size]).astype(jnp.int32)
    whole = lambda shape: pl.BlockSpec(shape, lambda i, at: (0,) * len(shape))
    part = pl.BlockSpec((size, width), lambda i, at: (at[0], at[1]))
    outs = ((NG, tokens, width), (NZ, size, 2 * width))
    return pl.pallas_call(
        prepare_kernel,
        grid_spec=pltpu.PrefetchScalarGridSpec(
            num_scalar_prefetch=1,
            grid=(1,),
            in_specs=[whole((tokens, width)), part, part, whole((1, width)), whole((1, width))],
            out_specs=[whole(shape) for shape in outs],
        ),
        out_shape=[jax.ShapeDtypeStruct(shape, BF) for shape in outs],
        name="prepare",
    )(at, queries, keys, values, query_gain[None, :], key_gain[None, :])


def split3(x):
    hi = x.astype(BF)
    rest = x - hi.astype(F32)
    mid = rest.astype(BF)
    lo = (rest - mid.astype(F32)).astype(BF)
    return hi, mid, lo


def attend_kernel(q_ref, own_ref, other_ref, out_ref):
    heads, rows, width = q_ref.shape
    factor = width ** (-0.5) * LOG2E
    keys = jnp.concatenate([own_ref[:, :width], other_ref[:, :width]], axis=0)
    values = jnp.concatenate([own_ref[:, width:], other_ref[:, width:]], axis=0)
    values = jnp.concatenate(
        [values.T, jnp.ones((STAT_ROWS, values.shape[0]), BF)], axis=0
    )
    row = lax.broadcasted_iota(jnp.int32, (STAT_ROWS, rows), 0)
    for head in range(heads):
        scores = lax.dot_general(
            keys, q_ref[head], (((1,), (1,)), ((), ())), preferred_element_type=F32
        )
        top = jnp.max(scores, axis=0, keepdims=True)
        weights = jnp.exp2((scores - top) * factor).astype(BF)
        summed = jnp.dot(values, weights, preferred_element_type=F32)
        total = summed[width : width + 1]
        out_ref[head, :width, :] = (summed[:width] * (1.0 / total)).astype(BF)
        stats = jnp.zeros((STAT_ROWS, rows), F32)
        for i, part in enumerate(split3(top * factor) + split3(total)):
            stats = jnp.where(row == i, part.astype(F32), stats)
        out_ref[head, width:, :] = stats.astype(BF)


def attend(q8, own, other):
    heads, rows, width = q8.shape
    return pl.pallas_call(
        attend_kernel,
        in_specs=[IN_VMEM] * 3,
        out_specs=IN_VMEM,
        out_shape=jax.ShapeDtypeStruct((heads, width + STAT_ROWS, rows), BF),
        compiler_params=grant(24),
        name="attend",
    )(q8, own, other)


def combine_kernel(parts_ref, out_ref):
    count = parts_ref.shape[0]
    width = out_ref.shape[1]
    tops, totals = [], []
    for j in range(count):
        s = parts_ref[j, width:, :].astype(F32)
        tops.append(s[0:1] + s[1:2] + s[2:3])
        totals.append(s[3:4] + s[4:5] + s[5:6])
    top = tops[0]
    for j in range(1, count):
        top = jnp.maximum(top, tops[j])
    shares = [totals[j] * jnp.exp2(tops[j] - top) for j in range(count)]
    whole = sum(shares[1:], shares[0])
    acc = jnp.zeros(out_ref.shape[1:], F32)
    for j in range(count):
        acc = acc + parts_ref[j, :width, :].astype(F32) * (shares[j] / whole)
    done = acc.astype(BF)
    for i in range(out_ref.shape[0]):
        out_ref[i] = done


def combine(parts):
    width = parts.shape[1] - STAT_ROWS
    return pl.pallas_call(
        combine_kernel,
        in_specs=[IN_VMEM],
        out_specs=IN_VMEM,
        out_shape=jax.ShapeDtypeStruct((NT, width, parts.shape[2]), BF),
        compiler_params=grant(16),
        name="combine",
    )(parts)


def deal_kernel(classes_ref, out_ref):
    for i, k in enumerate(COLOURS):
        out_ref[i] = classes_ref[k]


def deal(classes):
    return pl.pallas_call(
        deal_kernel,
        in_specs=[IN_VMEM],
        out_specs=IN_VMEM,
        out_shape=jax.ShapeDtypeStruct((NT, *classes.shape[1:]), BF),
        compiler_params=grant(16),
        name="deal",
    )(classes)


def collect_kernel(back_ref, out_ref):
    for k in range(NSHARE):
        total = None
        for i, colour in enumerate(COLOURS):
            if colour == k:
                part = back_ref[i].astype(F32)
                total = part if total is None else total + part
        out_ref[k] = total.astype(BF)


def collect(back):
    return pl.pallas_call(
        collect_kernel,
        in_specs=[IN_VMEM],
        out_specs=IN_VMEM,
        out_shape=jax.ShapeDtypeStruct((NSHARE, *back.shape[1:]), BF),
        compiler_params=grant(16),
        name="collect",
    )(back)


def pack_kernel(gate_ref, up_ref, down_ref, *out_refs):
    packed = jnp.concatenate([gate_ref[0].T, up_ref[0].T, down_ref[0]], axis=0)
    for half, out_ref in enumerate(out_refs):
        @pl.when(pl.program_id(0) == half)
        def _():
            out_ref[...] = packed


def pack(w_gate, w_up, w_down):
    _, depth, units = w_gate.shape
    wide = pl.BlockSpec((1, depth, SHARE), lambda i: (0, 0, i))
    shape = (3 * SHARE, depth)
    return pl.pallas_call(
        pack_kernel,
        grid=(units // SHARE,),
        in_specs=[wide, wide, pl.BlockSpec((1, SHARE, depth), lambda i: (0, i, 0))],
        out_specs=[pl.BlockSpec(shape, lambda i: (0, 0))] * 2,
        out_shape=[jax.ShapeDtypeStruct(shape, BF)] * 2,
        name="pack",
    )(w_gate, w_up, w_down)


def experts_kernel(rows_ref, *refs):
    pieces, (out_ref, held, acc, sems) = refs[:-4], refs[-4:]
    pairs = len(pieces) // 2
    copies = [
        pltpu.make_async_copy(
            pieces[2 * p + i].at[pl.ds(j * SHARE, SHARE)],
            held.at[p, j, pl.ds(i * SHARE, SHARE)],
            sems.at[p, j, i],
        )
        for p in range(pairs)
        for j in range(3)
        for i in range(2)
    ]
    for copy in copies[:12]:
        copy.start()
    across = (((1,), (1,)), ((), ()))
    for p in range(pairs):
        gate_up = []
        for j in range(2):
            for copy in copies[6 * p + 2 * j : 6 * p + 2 * j + 2]:
                copy.wait()
            gate_up.append(
                lax.dot_general(
                    rows_ref[...], held[p, j], across, preferred_element_type=F32
                )
            )
        gate, upper = gate_up
        hidden = (gate / (1.0 + jnp.exp(-gate)) * upper).astype(BF)
        for copy in copies[6 * p + 4 : 6 * p + 6]:
            copy.wait()
        for copy in copies[6 * (p + 2) : 6 * (p + 3)]:
            copy.start()
        part = jnp.dot(hidden, held[p, 2], preferred_element_type=F32)
        if p == 0:
            acc[...] = part
        elif p < pairs - 1:
            acc[...] += part
        else:
            out_ref[...] = (acc[...] + part).astype(BF)


def experts(rows, pieces):
    depth = rows.shape[1]
    return pl.pallas_call(
        experts_kernel,
        in_specs=[IN_VMEM] + [IN_HBM] * len(pieces),
        out_specs=IN_VMEM,
        out_shape=jax.ShapeDtypeStruct(rows.shape, BF),
        scratch_shapes=[
            pltpu.VMEM((len(pieces) // 2, 3, 2 * SHARE, depth), BF),
            pltpu.VMEM(rows.shape, F32),
            pltpu.SemaphoreType.DMA((len(pieces) // 2, 3, 2)),
        ],
        compiler_params=grant(32),
        name="experts",
    )(rows, *pieces)


def local(
    queries,
    keys,
    values,
    query_gain,
    key_gain,
    out_proj,
    expert_norm_scale,
    residual,
    routes,
    route_weights,
    w_gate,
    w_up,
    w_down,
):
    width = query_gain.shape[0]
    tok_sp = queries.shape[0]
    tok_dev, depth = residual.shape
    top = routes.shape[1]
    z, c = lax.axis_index("z"), lax.axis_index("c")
    yh, yl, x = lax.axis_index("yh"), lax.axis_index("yl"), lax.axis_index("x")
    start = (z * NC + c) * tok_sp

    q8, kv = prepare(
        queries, keys, values, query_gain, key_gain, yl * NX + x, yh, start
    )
    q8 = exchange(q8, GROUP)
    q8, kv = lax.optimization_barrier((q8, kv))
    kv_mine = exchange(kv, "z").reshape(-1, 2 * width)
    kv_other = swap_cores(kv_mine)

    packs = pack(w_gate, w_up, w_down)
    axes = ("x", ("yh", "yl"))
    left = [ring(p, axis, 1) for p, axis in zip(packs, axes)]
    right = [ring(p, axis, -1) for p, axis in zip(packs, axes)]
    far = [ring(p, axis, 1) for p, axis in zip(left, axes)]
    pieces = [*packs, *left, *right, *far]

    parts = attend(q8, kv_mine, kv_other)
    parts = exchange(parts, GROUP)
    attn_all = exchange(combine(parts), TP).reshape(NT * width, tok_sp)
    columns = lax.dot_general(
        attn_all, out_proj, (((0,), (0,)), ((), ())), preferred_element_type=F32
    ).astype(BF)
    projected = lax.all_to_all(columns, TP, split_axis=0, concat_axis=1, tiled=True)
    mixed = (residual.astype(F32) + projected.astype(F32)).astype(BF)
    mixed_f = mixed.astype(F32)
    normed = (
        mixed_f
        * lax.rsqrt(jnp.mean(mixed_f * mixed_f, axis=-1, keepdims=True) + EPS)
        * expert_norm_scale
    ).astype(BF)

    cap = max(2, 2 * tok_dev * top // (NZ * NC))
    tok = jnp.arange(tok_dev, dtype=jnp.int32)
    before = tok[None, :] < tok[:, None]
    place = jnp.arange(NZ * NC * cap, dtype=jnp.int32)
    expert_of, slot_of = place // cap, place % cap
    hits = []
    for k in range(top):
        mine = routes[:, k]
        slot = sum(
            jnp.sum(
                ((mine[:, None] == routes[:, j][None, :]) & before).astype(jnp.int32), axis=1
            )
            for j in range(top)
        )
        hits.append(
            (mine[:, None] == expert_of[None, :]) & (slot[:, None] == slot_of[None, :])
        )
    selector = sum(h.astype(BF) for h in hits)
    sent = lax.dot_general(
        selector, normed, (((0,), (0,)), ((), ())), preferred_element_type=F32
    ).astype(BF)
    arrived = exchange(sent, ("z", "c"))

    classes = arrived.reshape(NSHARE, NZ * NC * cap // NSHARE, depth)
    rows = exchange(deal(classes), TP)
    partial = experts(rows.reshape(-1, depth), pieces)
    back = exchange(partial.reshape(rows.shape), TP)
    picked_from = exchange(collect(back).reshape(arrived.shape), ("z", "c"))
    moe = sum(
        jnp.dot(hits[k].astype(BF), picked_from, preferred_element_type=F32)
        * route_weights[:, k][:, None]
        for k in range(top)
    )
    return (mixed_f + moe).astype(BF)


def solution(mesh):
    fine = Mesh(
        mesh.devices.reshape(NZ, NC, NYH, NYL, NX), ("z", "c", "yh", "yl", "x")
    )
    sp, both = ("z", "c"), ("z", "c", "yh", "yl", "x")
    placed = (
        P(sp, TP),
        P(sp, None),
        P(sp, None),
        P(),
        P(),
        P(None, TP),
        P(),
        P(both, None),
        P(both, None),
        P(both, None),
        P(sp, None, TP),
        P(sp, None, TP),
        P(sp, TP, None),
    )
    return jax.shard_map(
        local, mesh=fine, in_specs=placed, out_specs=P(both, None), check_vma=False
    )
```

```python
import math

import jax
import jax.numpy as jnp
from jax import lax
from jax.experimental import pallas as pl
from jax.experimental.pallas import tpu as pltpu
from jax.sharding import Mesh, PartitionSpec as P


GRID_W = 64
EPS = 1e-06
ROPE_BASE = 10000.0
LOG2E = 1.4426950408889634
BF = jnp.bfloat16
F32 = jnp.float32

NZ, NC, NYH, NYL, NX = 16, 2, 2, 2, 4
NY = NYH * NYL
NT = NY * NX
NG = NYL * NX
TP = ("yh", "yl", "x")
GROUP = ("yl", "x")
STAT_ROWS = 16
SHARE = 128
NSHARE = 4
COLOURS = tuple((i % NX + i // NX) % NSHARE for i in range(NT))


IN_VMEM = pl.BlockSpec(memory_space=pltpu.VMEM)
IN_HBM = pl.BlockSpec(memory_space=pltpu.HBM)


def grant(mib):
    return pltpu.CompilerParams(vmem_limit_bytes=mib * 1024 * 1024)


def exchange(blocks, axis):
    return lax.all_to_all(blocks, axis, split_axis=0, concat_axis=0, tiled=True)


def swap_cores(value):
    return lax.ppermute(value, "c", [(0, 1), (1, 0)])


def ring(value, axis, step):
    return lax.ppermute(value, axis, [(i, (i + step) % 4) for i in range(4)])


def turned(field, gain, start):
    count, width = field.shape
    quarter = width // 4
    f = field.astype(F32)
    f = f * lax.rsqrt(jnp.mean(f * f, axis=-1, keepdims=True) + EPS) * gain
    lane = lax.broadcasted_iota(jnp.int32, (count, width), 1)
    position = start + lax.broadcasted_iota(jnp.int32, (count, width), 0)
    coord = jnp.where(lane < 2 * quarter, position // GRID_W, position % GRID_W)
    step = (lane % quarter).astype(F32) / quarter
    angle = coord.astype(F32) * jnp.exp(step * (-math.log(ROPE_BASE)))
    first = lane % (2 * quarter) < quarter
    ahead = pltpu.roll(f, width - quarter, 1)
    behind = pltpu.roll(f, quarter, 1)
    other = jnp.where(first, -ahead, behind)
    return (f * jnp.cos(angle) + other * jnp.sin(angle)).astype(BF)


def prepare_kernel(at_ref, q_ref, k_ref, v_ref, q_gain_ref, k_gain_ref, q8_ref, kv_ref):
    q_rot = turned(q_ref[...], q_gain_ref[...], at_ref[2])
    for i in range(q8_ref.shape[0]):
        q8_ref[i] = q_rot
    k_rot = turned(k_ref[...], k_gain_ref[...], at_ref[3])
    both = jnp.concatenate([k_rot, v_ref[...]], axis=1)
    for i in range(kv_ref.shape[0]):
        kv_ref[i] = both


def prepare(queries, keys, values, query_gain, key_gain, block, head, start):
    tokens, width = queries.shape
    size = tokens // NG
    at = jnp.stack([block, head, start, start + block * size]).astype(jnp.int32)
    whole = lambda shape: pl.BlockSpec(shape, lambda i, at: (0,) * len(shape))
    part = pl.BlockSpec((size, width), lambda i, at: (at[0], at[1]))
    outs = ((NG, tokens, width), (NZ, size, 2 * width))
    return pl.pallas_call(
        prepare_kernel,
        grid_spec=pltpu.PrefetchScalarGridSpec(
            num_scalar_prefetch=1,
            grid=(1,),
            in_specs=[whole((tokens, width)), part, part, whole((1, width)), whole((1, width))],
            out_specs=[whole(shape) for shape in outs],
        ),
        out_shape=[jax.ShapeDtypeStruct(shape, BF) for shape in outs],
        name="prepare",
    )(at, queries, keys, values, query_gain[None, :], key_gain[None, :])


def split3(x):
    hi = x.astype(BF)
    rest = x - hi.astype(F32)
    mid = rest.astype(BF)
    lo = (rest - mid.astype(F32)).astype(BF)
    return hi, mid, lo


def attend_kernel(q_ref, own_ref, other_ref, out_ref):
    heads, rows, width = q_ref.shape
    factor = width ** (-0.5) * LOG2E
    keys = jnp.concatenate([own_ref[:, :width], other_ref[:, :width]], axis=0)
    values = jnp.concatenate([own_ref[:, width:], other_ref[:, width:]], axis=0)
    values = jnp.concatenate(
        [values.T, jnp.ones((STAT_ROWS, values.shape[0]), BF)], axis=0
    )
    row = lax.broadcasted_iota(jnp.int32, (STAT_ROWS, rows), 0)
    for head in range(heads):
        scores = lax.dot_general(
            keys, q_ref[head], (((1,), (1,)), ((), ())), preferred_element_type=F32
        )
        top = jnp.max(scores, axis=0, keepdims=True)
        weights = jnp.exp2((scores - top) * factor).astype(BF)
        summed = jnp.dot(values, weights, preferred_element_type=F32)
        total = summed[width : width + 1]
        out_ref[head, :width, :] = (summed[:width] * (1.0 / total)).astype(BF)
        stats = jnp.zeros((STAT_ROWS, rows), F32)
        for i, part in enumerate(split3(top * factor) + split3(total)):
            stats = jnp.where(row == i, part.astype(F32), stats)
        out_ref[head, width:, :] = stats.astype(BF)


def attend(q8, own, other):
    heads, rows, width = q8.shape
    return pl.pallas_call(
        attend_kernel,
        in_specs=[IN_VMEM] * 3,
        out_specs=IN_VMEM,
        out_shape=jax.ShapeDtypeStruct((heads, width + STAT_ROWS, rows), BF),
        compiler_params=grant(24),
        name="attend",
    )(q8, own, other)


def combine_kernel(parts_ref, out_ref):
    count = parts_ref.shape[0]
    width = out_ref.shape[1]
    tops, totals = [], []
    for j in range(count):
        s = parts_ref[j, width:, :].astype(F32)
        tops.append(s[0:1] + s[1:2] + s[2:3])
        totals.append(s[3:4] + s[4:5] + s[5:6])
    top = tops[0]
    for j in range(1, count):
        top = jnp.maximum(top, tops[j])
    shares = [totals[j] * jnp.exp2(tops[j] - top) for j in range(count)]
    whole = sum(shares[1:], shares[0])
    acc = jnp.zeros(out_ref.shape[1:], F32)
    for j in range(count):
        acc = acc + parts_ref[j, :width, :].astype(F32) * (shares[j] / whole)
    done = acc.astype(BF)
    for i in range(out_ref.shape[0]):
        out_ref[i] = done


def combine(parts):
    width = parts.shape[1] - STAT_ROWS
    return pl.pallas_call(
        combine_kernel,
        in_specs=[IN_VMEM],
        out_specs=IN_VMEM,
        out_shape=jax.ShapeDtypeStruct((NT, width, parts.shape[2]), BF),
        compiler_params=grant(16),
        name="combine",
    )(parts)


def deal_kernel(classes_ref, out_ref):
    for i, k in enumerate(COLOURS):
        out_ref[i] = classes_ref[k]


def deal(classes):
    return pl.pallas_call(
        deal_kernel,
        in_specs=[IN_VMEM],
        out_specs=IN_VMEM,
        out_shape=jax.ShapeDtypeStruct((NT, *classes.shape[1:]), BF),
        compiler_params=grant(16),
        name="deal",
    )(classes)


def collect_kernel(back_ref, out_ref):
    for k in range(NSHARE):
        total = None
        for i, colour in enumerate(COLOURS):
            if colour == k:
                part = back_ref[i].astype(F32)
                total = part if total is None else total + part
        out_ref[k] = total.astype(BF)


def collect(back):
    return pl.pallas_call(
        collect_kernel,
        in_specs=[IN_VMEM],
        out_specs=IN_VMEM,
        out_shape=jax.ShapeDtypeStruct((NSHARE, *back.shape[1:]), BF),
        compiler_params=grant(16),
        name="collect",
    )(back)


def pack_kernel(gate_ref, up_ref, down_ref, *out_refs):
    gate_up = jnp.concatenate([gate_ref[0].T, up_ref[0].T], axis=0)
    for half in range(2):
        @pl.when(pl.program_id(0) == half)
        def _():
            out_refs[half][...] = gate_up
            out_refs[2 + half][...] = down_ref[0]


def pack(w_gate, w_up, w_down):
    _, depth, units = w_gate.shape
    wide = pl.BlockSpec((1, depth, SHARE), lambda i: (0, 0, i))
    shapes = [(2 * SHARE, depth)] * 2 + [(SHARE, depth)] * 2
    outs = pl.pallas_call(
        pack_kernel,
        grid=(units // SHARE,),
        in_specs=[wide, wide, pl.BlockSpec((1, SHARE, depth), lambda i: (0, i, 0))],
        out_specs=[pl.BlockSpec(shape, lambda i: (0, 0)) for shape in shapes],
        out_shape=[jax.ShapeDtypeStruct(shape, BF) for shape in shapes],
        name="pack",
    )(w_gate, w_up, w_down)
    return outs[:2], outs[2:]


def experts_kernel(rows_ref, *refs):
    pieces, (out_ref, ups, downs, acc, sems) = refs[:-5], refs[-5:]
    count = len(pieces) // 4
    copies = []
    for p in range(count):
        for i in range(2):
            copies.append((pieces[2 * p + i], ups.at[p, pl.ds(2 * i * SHARE, 2 * SHARE)]))
        for i in range(2):
            copies.append(
                (pieces[2 * (count + p) + i], downs.at[p, pl.ds(i * SHARE, SHARE)])
            )
    copies = [
        pltpu.make_async_copy(source, target, sems.at[i])
        for i, (source, target) in enumerate(copies)
    ]
    for copy in copies[:8]:
        copy.start()
    for p in range(count):
        for copy in copies[4 * p : 4 * p + 2]:
            copy.wait()
        both = lax.dot_general(
            ups[p], rows_ref[...], (((1,), (1,)), ((), ())), preferred_element_type=F32
        )
        for copy in copies[4 * (p + 2) : 4 * (p + 3)]:
            copy.start()
        hidden = []
        for i in range(2):
            gate = both[2 * i * SHARE : (2 * i + 1) * SHARE]
            upper = both[(2 * i + 1) * SHARE : (2 * i + 2) * SHARE]
            hidden.append((gate / (1.0 + jnp.exp(-gate)) * upper).astype(BF))
        for copy in copies[4 * p + 2 : 4 * p + 4]:
            copy.wait()
        part = lax.dot_general(
            jnp.concatenate(hidden, axis=0),
            downs[p],
            (((0,), (0,)), ((), ())),
            preferred_element_type=F32,
        )
        if p == 0:
            acc[...] = part
        elif p < count - 1:
            acc[...] += part
        else:
            out_ref[...] = (acc[...] + part).astype(BF)


def experts(rows, pieces):
    count, depth = len(pieces) // 4, rows.shape[1]
    return pl.pallas_call(
        experts_kernel,
        in_specs=[IN_VMEM] + [IN_HBM] * len(pieces),
        out_specs=IN_VMEM,
        out_shape=jax.ShapeDtypeStruct(rows.shape, BF),
        scratch_shapes=[
            pltpu.VMEM((count, 4 * SHARE, depth), BF),
            pltpu.VMEM((count, 2 * SHARE, depth), BF),
            pltpu.VMEM(rows.shape, F32),
            pltpu.SemaphoreType.DMA((len(pieces),)),
        ],
        compiler_params=grant(54),
        name="experts",
    )(rows, *pieces)


def local(
    queries,
    keys,
    values,
    query_gain,
    key_gain,
    out_proj,
    expert_norm_scale,
    residual,
    routes,
    route_weights,
    w_gate,
    w_up,
    w_down,
):
    width = query_gain.shape[0]
    tok_sp = queries.shape[0]
    tok_dev, depth = residual.shape
    top = routes.shape[1]
    z, c = lax.axis_index("z"), lax.axis_index("c")
    yh, yl, x = lax.axis_index("yh"), lax.axis_index("yl"), lax.axis_index("x")
    start = (z * NC + c) * tok_sp

    q8, kv = prepare(
        queries, keys, values, query_gain, key_gain, yl * NX + x, yh, start
    )
    q8 = exchange(q8, GROUP)
    q8, kv = lax.optimization_barrier((q8, kv))
    kv_mine = exchange(kv, "z").reshape(-1, 2 * width)
    kv_other = swap_cores(kv_mine)

    ups, downs = pack(w_gate, w_up, w_down)
    axes = ("x", ("yh", "yl"))
    pieces = []
    for packs in (ups, downs):
        left = [ring(p, axis, 1) for p, axis in zip(packs, axes)]
        right = [ring(p, axis, -1) for p, axis in zip(packs, axes)]
        last = [ring(p, axis, 1) for p, axis in zip(left, axes)]
        pieces += [*packs, *left, *right, *last]

    parts = attend(q8, kv_mine, kv_other)
    parts = exchange(parts, GROUP)
    attn_all = exchange(combine(parts), TP).reshape(NT * width, tok_sp)
    columns = lax.dot_general(
        attn_all, out_proj, (((0,), (0,)), ((), ())), preferred_element_type=F32
    ).astype(BF)
    projected = lax.all_to_all(columns, TP, split_axis=0, concat_axis=1, tiled=True)
    mixed = (residual.astype(F32) + projected.astype(F32)).astype(BF)
    mixed_f = mixed.astype(F32)
    normed = (
        mixed_f
        * lax.rsqrt(jnp.mean(mixed_f * mixed_f, axis=-1, keepdims=True) + EPS)
        * expert_norm_scale
    ).astype(BF)

    cap = max(2, 2 * tok_dev * top // (NZ * NC))
    tok = jnp.arange(tok_dev, dtype=jnp.int32)
    before = tok[None, :] < tok[:, None]
    place = jnp.arange(NZ * NC * cap, dtype=jnp.int32)
    expert_of, slot_of = place // cap, place % cap
    hits = []
    for k in range(top):
        mine = routes[:, k]
        slot = sum(
            jnp.sum(
                ((mine[:, None] == routes[:, j][None, :]) & before).astype(jnp.int32), axis=1
            )
            for j in range(top)
        )
        hits.append(
            (mine[:, None] == expert_of[None, :]) & (slot[:, None] == slot_of[None, :])
        )
    selector = sum(h.astype(BF) for h in hits)
    sent = lax.dot_general(
        selector, normed, (((0,), (0,)), ((), ())), preferred_element_type=F32
    ).astype(BF)
    arrived = exchange(sent, ("z", "c"))

    classes = arrived.reshape(NSHARE, NZ * NC * cap // NSHARE, depth)
    rows = exchange(deal(classes), TP)
    partial = experts(rows.reshape(-1, depth), pieces)
    back = exchange(partial.reshape(rows.shape), TP)
    picked_from = exchange(collect(back).reshape(arrived.shape), ("z", "c"))
    moe = sum(
        jnp.dot(hits[k].astype(BF), picked_from, preferred_element_type=F32)
        * route_weights[:, k][:, None]
        for k in range(top)
    )
    return (mixed_f + moe).astype(BF)


def solution(mesh):
    fine = Mesh(
        mesh.devices.reshape(NZ, NC, NYH, NYL, NX), ("z", "c", "yh", "yl", "x")
    )
    sp, both = ("z", "c"), ("z", "c", "yh", "yl", "x")
    placed = (
        P(sp, TP),
        P(sp, None),
        P(sp, None),
        P(),
        P(),
        P(None, TP),
        P(),
        P(both, None),
        P(both, None),
        P(both, None),
        P(sp, None, TP),
        P(sp, None, TP),
        P(sp, TP, None),
    )
    return jax.shard_map(
        local, mesh=fine, in_specs=placed, out_specs=P(both, None), check_vma=False
    )
```

```python
import math

import jax
import jax.numpy as jnp
from jax import lax
from jax.experimental import pallas as pl
from jax.experimental.pallas import tpu as pltpu
from jax.sharding import Mesh, PartitionSpec as P


GRID_W = 64
EPS = 1e-06
ROPE_BASE = 10000.0
LOG2E = 1.4426950408889634
BF = jnp.bfloat16
F32 = jnp.float32

NZ, NC, NYH, NYL, NX = 16, 2, 2, 2, 4
NY = NYH * NYL
NT = NY * NX
NG = NYL * NX
TP = ("yh", "yl", "x")
GROUP = ("yl", "x")
STAT_ROWS = 16
EXPERT_GRANT = 46
SHARE = 128
NSHARE = 4
COLOURS = tuple((i % NX + i // NX) % NSHARE for i in range(NT))


IN_VMEM = pl.BlockSpec(memory_space=pltpu.VMEM)
IN_HBM = pl.BlockSpec(memory_space=pltpu.HBM)


def grant(mib):
    return pltpu.CompilerParams(vmem_limit_bytes=mib * 1024 * 1024)


def exchange(blocks, axis):
    return lax.all_to_all(blocks, axis, split_axis=0, concat_axis=0, tiled=True)


def swap_cores(value):
    return lax.ppermute(value, "c", [(0, 1), (1, 0)])


def ring(value, axis, step):
    return lax.ppermute(value, axis, [(i, (i + step) % 4) for i in range(4)])


def turned(field, gain, start):
    count, width = field.shape
    quarter = width // 4
    f = field.astype(F32)
    f = f * lax.rsqrt(jnp.mean(f * f, axis=-1, keepdims=True) + EPS) * gain
    lane = lax.broadcasted_iota(jnp.int32, (count, width), 1)
    position = start + lax.broadcasted_iota(jnp.int32, (count, width), 0)
    coord = jnp.where(lane < 2 * quarter, position // GRID_W, position % GRID_W)
    step = (lane % quarter).astype(F32) / quarter
    angle = coord.astype(F32) * jnp.exp(step * (-math.log(ROPE_BASE)))
    first = lane % (2 * quarter) < quarter
    ahead = pltpu.roll(f, width - quarter, 1)
    behind = pltpu.roll(f, quarter, 1)
    other = jnp.where(first, -ahead, behind)
    return (f * jnp.cos(angle) + other * jnp.sin(angle)).astype(BF)


def prepare_kernel(at_ref, q_ref, k_ref, v_ref, q_gain_ref, k_gain_ref, q8_ref, kv_ref):
    q_rot = turned(q_ref[...], q_gain_ref[...], at_ref[2])
    for i in range(q8_ref.shape[0]):
        q8_ref[i] = q_rot
    k_rot = turned(k_ref[...], k_gain_ref[...], at_ref[3])
    both = jnp.concatenate([k_rot, v_ref[...]], axis=1)
    for i in range(kv_ref.shape[0]):
        kv_ref[i] = both


def prepare(queries, keys, values, query_gain, key_gain, block, head, start):
    tokens, width = queries.shape
    size = tokens // NG
    at = jnp.stack([block, head, start, start + block * size]).astype(jnp.int32)
    whole = lambda shape: pl.BlockSpec(shape, lambda i, at: (0,) * len(shape))
    part = pl.BlockSpec((size, width), lambda i, at: (at[0], at[1]))
    outs = ((NG, tokens, width), (NZ, size, 2 * width))
    return pl.pallas_call(
        prepare_kernel,
        grid_spec=pltpu.PrefetchScalarGridSpec(
            num_scalar_prefetch=1,
            grid=(1,),
            in_specs=[whole((tokens, width)), part, part, whole((1, width)), whole((1, width))],
            out_specs=[whole(shape) for shape in outs],
        ),
        out_shape=[jax.ShapeDtypeStruct(shape, BF) for shape in outs],
        name="prepare",
    )(at, queries, keys, values, query_gain[None, :], key_gain[None, :])


def split3(x):
    hi = x.astype(BF)
    rest = x - hi.astype(F32)
    mid = rest.astype(BF)
    lo = (rest - mid.astype(F32)).astype(BF)
    return hi, mid, lo


def attend_kernel(q_ref, own_ref, other_ref, out_ref, scores_ref):
    heads, rows, width = q_ref.shape
    factor = width ** (-0.5) * LOG2E
    keys = jnp.concatenate([own_ref[:, :width], other_ref[:, :width]], axis=0)
    values = jnp.concatenate([own_ref[:, width:], other_ref[:, width:]], axis=0)
    values = jnp.concatenate(
        [values.T, jnp.ones((STAT_ROWS, values.shape[0]), BF)], axis=0
    )
    row = lax.broadcasted_iota(jnp.int32, (STAT_ROWS, rows), 0)

    def score(head):
        scores_ref[head % 2] = lax.dot_general(
            keys, q_ref[head], (((1,), (1,)), ((), ())), preferred_element_type=F32
        )

    score(0)
    for head in range(heads):
        if head + 1 < heads:
            score(head + 1)
        scores = scores_ref[head % 2]
        top = jnp.max(scores, axis=0, keepdims=True)
        weights = jnp.exp2((scores - top) * factor).astype(BF)
        summed = jnp.dot(values, weights, preferred_element_type=F32)
        total = summed[width : width + 1]
        out_ref[head, :width, :] = (summed[:width] * (1.0 / total)).astype(BF)
        stats = jnp.zeros((STAT_ROWS, rows), F32)
        for i, part in enumerate(split3(top * factor) + split3(total)):
            stats = jnp.where(row == i, part.astype(F32), stats)
        out_ref[head, width:, :] = stats.astype(BF)


def attend(q8, own, other):
    heads, rows, width = q8.shape
    return pl.pallas_call(
        attend_kernel,
        in_specs=[IN_VMEM] * 3,
        out_specs=IN_VMEM,
        out_shape=jax.ShapeDtypeStruct((heads, width + STAT_ROWS, rows), BF),
        scratch_shapes=[pltpu.VMEM((2, NC * own.shape[0], rows), F32)],
        compiler_params=grant(24),
        name="attend",
    )(q8, own, other)


def combine_kernel(parts_ref, out_ref):
    count = parts_ref.shape[0]
    width = out_ref.shape[1]
    tops, totals = [], []
    for j in range(count):
        s = parts_ref[j, width:, :].astype(F32)
        tops.append(s[0:1] + s[1:2] + s[2:3])
        totals.append(s[3:4] + s[4:5] + s[5:6])
    top = tops[0]
    for j in range(1, count):
        top = jnp.maximum(top, tops[j])
    shares = [totals[j] * jnp.exp2(tops[j] - top) for j in range(count)]
    whole = sum(shares[1:], shares[0])
    acc = jnp.zeros(out_ref.shape[1:], F32)
    for j in range(count):
        acc = acc + parts_ref[j, :width, :].astype(F32) * (shares[j] / whole)
    done = acc.astype(BF)
    for i in range(out_ref.shape[0]):
        out_ref[i] = done


def combine(parts):
    width = parts.shape[1] - STAT_ROWS
    return pl.pallas_call(
        combine_kernel,
        in_specs=[IN_VMEM],
        out_specs=IN_VMEM,
        out_shape=jax.ShapeDtypeStruct((NT, width, parts.shape[2]), BF),
        compiler_params=grant(16),
        name="combine",
    )(parts)


def deal_kernel(classes_ref, out_ref):
    for i, k in enumerate(COLOURS):
        out_ref[i] = classes_ref[k]


def deal(classes):
    return pl.pallas_call(
        deal_kernel,
        in_specs=[IN_VMEM],
        out_specs=IN_VMEM,
        out_shape=jax.ShapeDtypeStruct((NT, *classes.shape[1:]), BF),
        compiler_params=grant(16),
        name="deal",
    )(classes)


def collect_kernel(back_ref, out_ref):
    for k in range(NSHARE):
        total = None
        for i, colour in enumerate(COLOURS):
            if colour == k:
                part = back_ref[i].astype(F32)
                total = part if total is None else total + part
        out_ref[k] = total.astype(BF)


def collect(back):
    return pl.pallas_call(
        collect_kernel,
        in_specs=[IN_VMEM],
        out_specs=IN_VMEM,
        out_shape=jax.ShapeDtypeStruct((NSHARE, *back.shape[1:]), BF),
        compiler_params=grant(16),
        name="collect",
    )(back)


def pack_kernel(gate_ref, up_ref, down_ref, *out_refs):
    gate_up = jnp.concatenate([gate_ref[0].T, up_ref[0].T], axis=0)
    for half in range(2):
        @pl.when(pl.program_id(0) == half)
        def _():
            out_refs[half][...] = gate_up
            out_refs[2 + half][...] = down_ref[0]


def pack(w_gate, w_up, w_down):
    _, depth, units = w_gate.shape
    wide = pl.BlockSpec((1, depth, SHARE), lambda i: (0, 0, i))
    shapes = [(2 * SHARE, depth)] * 2 + [(SHARE, depth)] * 2
    outs = pl.pallas_call(
        pack_kernel,
        grid=(units // SHARE,),
        in_specs=[wide, wide, pl.BlockSpec((1, SHARE, depth), lambda i: (0, i, 0))],
        out_specs=[pl.BlockSpec(shape, lambda i: (0, 0)) for shape in shapes],
        out_shape=[jax.ShapeDtypeStruct(shape, BF) for shape in shapes],
        name="pack",
    )(w_gate, w_up, w_down)
    return outs[:2], outs[2:]


def experts_kernel(rows_ref, *refs):
    pieces, (out_ref, held, acc, sems) = refs[:-4], refs[-4:]
    pairs = len(pieces) // 4
    ups, downs = pieces[: 2 * pairs], pieces[2 * pairs :]
    copies = []
    for p in range(pairs):
        for j in range(3):
            for i in range(2):
                source = downs[2 * p + i]
                if j < 2:
                    source = ups[2 * p + i].at[pl.ds(j * SHARE, SHARE)]
                copies.append(
                    pltpu.make_async_copy(
                        source, held.at[p, j, pl.ds(i * SHARE, SHARE)], sems.at[p, j, i]
                    )
                )
    for copy in copies[:12]:
        copy.start()
    across = (((1,), (1,)), ((), ()))
    for p in range(pairs):
        gate_up = []
        for j in range(2):
            for copy in copies[6 * p + 2 * j : 6 * p + 2 * j + 2]:
                copy.wait()
            gate_up.append(
                lax.dot_general(
                    rows_ref[...], held[p, j], across, preferred_element_type=F32
                )
            )
        gate, upper = gate_up
        hidden = (gate / (1.0 + jnp.exp(-gate)) * upper).astype(BF)
        for copy in copies[6 * p + 4 : 6 * p + 6]:
            copy.wait()
        for copy in copies[6 * (p + 2) : 6 * (p + 3)]:
            copy.start()
        part = jnp.dot(hidden, held[p, 2], preferred_element_type=F32)
        if p == 0:
            acc[...] = part
        elif p < pairs - 1:
            acc[...] += part
        else:
            out_ref[...] = (acc[...] + part).astype(BF)


def experts(rows, pieces):
    pairs, depth = len(pieces) // 4, rows.shape[1]
    return pl.pallas_call(
        experts_kernel,
        in_specs=[IN_VMEM] + [IN_HBM] * len(pieces),
        out_specs=IN_VMEM,
        out_shape=jax.ShapeDtypeStruct(rows.shape, BF),
        scratch_shapes=[
            pltpu.VMEM((pairs, 3, 2 * SHARE, depth), BF),
            pltpu.VMEM(rows.shape, F32),
            pltpu.SemaphoreType.DMA((pairs, 3, 2)),
        ],
        compiler_params=grant(EXPERT_GRANT),
        name="experts",
    )(rows, *pieces)


def local(
    queries,
    keys,
    values,
    query_gain,
    key_gain,
    out_proj,
    expert_norm_scale,
    residual,
    routes,
    route_weights,
    w_gate,
    w_up,
    w_down,
):
    width = query_gain.shape[0]
    tok_sp = queries.shape[0]
    tok_dev, depth = residual.shape
    top = routes.shape[1]
    z, c = lax.axis_index("z"), lax.axis_index("c")
    yh, yl, x = lax.axis_index("yh"), lax.axis_index("yl"), lax.axis_index("x")
    start = (z * NC + c) * tok_sp

    q8, kv = prepare(
        queries, keys, values, query_gain, key_gain, yl * NX + x, yh, start
    )
    q8 = exchange(q8, GROUP)
    q8, kv = lax.optimization_barrier((q8, kv))
    kv_mine = exchange(kv, "z").reshape(-1, 2 * width)
    kv_other = swap_cores(kv_mine)

    ups, downs = pack(w_gate, w_up, w_down)
    axes = ("x", ("yh", "yl"))
    pieces = []
    for packs in (ups, downs):
        left = [ring(p, axis, 1) for p, axis in zip(packs, axes)]
        right = [ring(p, axis, -1) for p, axis in zip(packs, axes)]
        last = [ring(p, axis, 1) for p, axis in zip(left, axes)]
        pieces += [*packs, *left, *right, *last]

    parts = attend(q8, kv_mine, kv_other)
    parts = exchange(parts, GROUP)
    attn_all = exchange(combine(parts), TP).reshape(NT * width, tok_sp)
    columns = lax.dot_general(
        attn_all, out_proj, (((0,), (0,)), ((), ())), preferred_element_type=F32
    ).astype(BF)
    projected = lax.all_to_all(columns, TP, split_axis=0, concat_axis=1, tiled=True)
    mixed = (residual.astype(F32) + projected.astype(F32)).astype(BF)
    mixed_f = mixed.astype(F32)
    normed = (
        mixed_f
        * lax.rsqrt(jnp.mean(mixed_f * mixed_f, axis=-1, keepdims=True) + EPS)
        * expert_norm_scale
    ).astype(BF)

    cap = max(2, 2 * tok_dev * top // (NZ * NC))
    tok = jnp.arange(tok_dev, dtype=jnp.int32)
    before = tok[None, :] < tok[:, None]
    place = jnp.arange(NZ * NC * cap, dtype=jnp.int32)
    expert_of, slot_of = place // cap, place % cap
    hits = []
    for k in range(top):
        mine = routes[:, k]
        slot = sum(
            jnp.sum(
                ((mine[:, None] == routes[:, j][None, :]) & before).astype(jnp.int32), axis=1
            )
            for j in range(top)
        )
        hits.append(
            (mine[:, None] == expert_of[None, :]) & (slot[:, None] == slot_of[None, :])
        )
    selector = sum(h.astype(BF) for h in hits)
    sent = lax.dot_general(
        selector, normed, (((0,), (0,)), ((), ())), preferred_element_type=F32
    ).astype(BF)
    arrived = exchange(sent, ("z", "c"))

    classes = arrived.reshape(NSHARE, NZ * NC * cap // NSHARE, depth)
    rows = exchange(deal(classes), TP)
    partial = experts(rows.reshape(-1, depth), pieces)
    back = exchange(partial.reshape(rows.shape), TP)
    picked_from = exchange(collect(back).reshape(arrived.shape), ("z", "c"))
    moe = sum(
        jnp.dot(hits[k].astype(BF), picked_from, preferred_element_type=F32)
        * route_weights[:, k][:, None]
        for k in range(top)
    )
    return (mixed_f + moe).astype(BF)


def solution(mesh):
    fine = Mesh(
        mesh.devices.reshape(NZ, NC, NYH, NYL, NX), ("z", "c", "yh", "yl", "x")
    )
    sp, both = ("z", "c"), ("z", "c", "yh", "yl", "x")
    placed = (
        P(sp, TP),
        P(sp, None),
        P(sp, None),
        P(),
        P(),
        P(None, TP),
        P(),
        P(both, None),
        P(both, None),
        P(both, None),
        P(sp, None, TP),
        P(sp, None, TP),
        P(sp, TP, None),
    )
    return jax.shard_map(
        local, mesh=fine, in_specs=placed, out_specs=P(both, None), check_vma=False
    )
```

```python
import math

import jax
import jax.numpy as jnp
from jax import lax
from jax.experimental import pallas as pl
from jax.experimental.pallas import tpu as pltpu
from jax.sharding import Mesh, PartitionSpec as P


GRID_W = 64
EPS = 1e-06
ROPE_BASE = 10000.0
LOG2E = 1.4426950408889634
BF = jnp.bfloat16
F32 = jnp.float32

NZ, NC, NYH, NYL, NX = 16, 2, 2, 2, 4
NY = NYH * NYL
NT = NY * NX
NG = NYL * NX
TP = ("yh", "yl", "x")
GROUP = ("yl", "x")
STAT_ROWS = 16
FOLD = 8
EXPERT_GRANT = 46
SHARE = 128
NSHARE = 4
COLOURS = tuple((i % NX + i // NX) % NSHARE for i in range(NT))


IN_VMEM = pl.BlockSpec(memory_space=pltpu.VMEM)
IN_HBM = pl.BlockSpec(memory_space=pltpu.HBM)


def grant(mib):
    return pltpu.CompilerParams(vmem_limit_bytes=mib * 1024 * 1024)


def exchange(blocks, axis):
    return lax.all_to_all(blocks, axis, split_axis=0, concat_axis=0, tiled=True)


def swap_cores(value):
    return lax.ppermute(value, "c", [(0, 1), (1, 0)])


def ring(value, axis, step):
    return lax.ppermute(value, axis, [(i, (i + step) % 4) for i in range(4)])


def turned(field, gain, start):
    count, width = field.shape
    quarter = width // 4
    f = field.astype(F32)
    f = f * lax.rsqrt(jnp.mean(f * f, axis=-1, keepdims=True) + EPS) * gain
    lane = lax.broadcasted_iota(jnp.int32, (count, width), 1)
    position = start + lax.broadcasted_iota(jnp.int32, (count, width), 0)
    coord = jnp.where(lane < 2 * quarter, position // GRID_W, position % GRID_W)
    step = (lane % quarter).astype(F32) / quarter
    angle = coord.astype(F32) * jnp.exp(step * (-math.log(ROPE_BASE)))
    first = lane % (2 * quarter) < quarter
    ahead = pltpu.roll(f, width - quarter, 1)
    behind = pltpu.roll(f, quarter, 1)
    other = jnp.where(first, -ahead, behind)
    return (f * jnp.cos(angle) + other * jnp.sin(angle)).astype(BF)


def queries_kernel(start_ref, q_ref, gain_ref, out_ref):
    q_rot = turned(q_ref[...], gain_ref[...], start_ref[0])
    for i in range(out_ref.shape[0]):
        out_ref[i] = q_rot


def prepare_queries(queries, gain, start):
    return pl.pallas_call(
        queries_kernel,
        in_specs=[pl.BlockSpec(memory_space=pltpu.SMEM), IN_VMEM, IN_VMEM],
        out_specs=IN_VMEM,
        out_shape=jax.ShapeDtypeStruct((NG, *queries.shape), BF),
        name="prepare_queries",
    )(start.reshape(1), queries, gain[None, :])


def keys_kernel(at_ref, k_ref, v_ref, gain_ref, out_ref):
    k_rot = turned(k_ref[...], gain_ref[...], at_ref[2])
    both = jnp.concatenate([k_rot, v_ref[...]], axis=1)
    for i in range(out_ref.shape[0]):
        out_ref[i] = both


def prepare_keys(keys, values, gain, block, head, start):
    width = gain.shape[0]
    size = keys.shape[0] // NG
    at = jnp.stack([block, head, start + block * size]).astype(jnp.int32)
    part = pl.BlockSpec((size, width), lambda i, at: (at[0], at[1]))
    out = (NZ, size, 2 * width)
    return pl.pallas_call(
        keys_kernel,
        grid_spec=pltpu.PrefetchScalarGridSpec(
            num_scalar_prefetch=1,
            grid=(1,),
            in_specs=[part, part, pl.BlockSpec((1, width), lambda i, at: (0, 0))],
            out_specs=pl.BlockSpec(out, lambda i, at: (0, 0, 0)),
        ),
        out_shape=jax.ShapeDtypeStruct(out, BF),
        name="prepare_keys",
    )(at, keys, values, gain[None, :])


def split3(x):
    hi = x.astype(BF)
    rest = x - hi.astype(F32)
    mid = rest.astype(BF)
    lo = (rest - mid.astype(F32)).astype(BF)
    return hi, mid, lo


def attend_kernel(q_ref, own_ref, other_ref, out_ref, scores_ref):
    heads, rows, width = q_ref.shape
    factor = width ** (-0.5) * LOG2E
    keys = jnp.concatenate([own_ref[:, :width], other_ref[:, :width]], axis=0)
    values = jnp.concatenate([own_ref[:, width:], other_ref[:, width:]], axis=0)
    values = jnp.concatenate(
        [values.T, jnp.ones((STAT_ROWS, values.shape[0]), BF)], axis=0
    )
    row = lax.broadcasted_iota(jnp.int32, (STAT_ROWS, rows), 0)

    def score(head):
        scores_ref[head % 2] = lax.dot_general(
            keys, q_ref[head], (((1,), (1,)), ((), ())), preferred_element_type=F32
        )

    score(0)
    for head in range(heads):
        if head + 1 < heads:
            score(head + 1)
        scores = scores_ref[head % 2]
        top = jnp.max(scores, axis=0, keepdims=True)
        weights = jnp.exp2((scores - top) * factor).astype(BF)
        summed = jnp.dot(values, weights, preferred_element_type=F32)
        total = summed[width : width + 1]
        out_ref[head, :width, :] = (summed[:width] * (1.0 / total)).astype(BF)
        stats = jnp.zeros((STAT_ROWS, rows), F32)
        for i, part in enumerate(split3(top * factor) + split3(total)):
            stats = jnp.where(row == i, part.astype(F32), stats)
        out_ref[head, width:, :] = stats.astype(BF)


def attend(q8, own, other):
    heads, rows, width = q8.shape
    return pl.pallas_call(
        attend_kernel,
        in_specs=[IN_VMEM] * 3,
        out_specs=IN_VMEM,
        out_shape=jax.ShapeDtypeStruct((heads, width + STAT_ROWS, rows), BF),
        scratch_shapes=[pltpu.VMEM((2, NC * own.shape[0], rows), F32)],
        compiler_params=grant(24),
        name="attend",
    )(q8, own, other)


def combine_kernel(parts_ref, out_ref):
    count = parts_ref.shape[0]
    width = out_ref.shape[1]
    tops, totals = [], []
    for j in range(count):
        s = parts_ref[j, width:, :].astype(F32)
        tops.append(s[0:1] + s[1:2] + s[2:3])
        totals.append(s[3:4] + s[4:5] + s[5:6])
    top = tops[0]
    for j in range(1, count):
        top = jnp.maximum(top, tops[j])
    shares = [totals[j] * jnp.exp2(tops[j] - top) for j in range(count)]
    whole = sum(shares[1:], shares[0])
    acc = jnp.zeros(out_ref.shape[1:], F32)
    for j in range(count):
        acc = acc + parts_ref[j, :width, :].astype(F32) * (shares[j] / whole)
    done = acc.astype(BF)
    for i in range(out_ref.shape[0]):
        out_ref[i] = done


def combine(parts):
    width = parts.shape[1] - STAT_ROWS
    return pl.pallas_call(
        combine_kernel,
        in_specs=[IN_VMEM],
        out_specs=IN_VMEM,
        out_shape=jax.ShapeDtypeStruct((NT, width, parts.shape[2]), BF),
        compiler_params=grant(16),
        name="combine",
    )(parts)


def folded(rows):
    width = rows.shape[1] // FOLD
    return jnp.concatenate(
        [rows[:, j * width : (j + 1) * width] for j in range(FOLD)], axis=0
    )


def picking(outs, ins, source_of):
    i = lax.broadcasted_iota(jnp.int32, (outs, ins), 0)
    r = lax.broadcasted_iota(jnp.int32, (outs, ins), 1)
    return jnp.where(r == source_of(i), 1.0, 0.0).astype(BF)


def mix_kernel(projected_ref, residual_ref, scale_ref, selector_ref, mixed_ref, sent_ref):
    projected = jnp.concatenate(
        [projected_ref[i].astype(F32) for i in range(projected_ref.shape[0])], axis=1
    )
    mixed = (residual_ref[...].astype(F32) + projected).astype(BF)
    mixed_ref[...] = mixed
    mixed = mixed.astype(F32)
    mean = jnp.mean(mixed * mixed, axis=-1, keepdims=True)
    normed = (mixed * lax.rsqrt(mean + EPS) * scale_ref[...]).astype(BF)
    sent_ref[...] = jnp.dot(
        selector_ref[...], folded(normed), preferred_element_type=F32
    ).astype(BF)


def mix(projected, residual, scale, selector):
    shape = (selector.shape[0], residual.shape[1] // FOLD)
    return pl.pallas_call(
        mix_kernel,
        in_specs=[IN_VMEM] * 4,
        out_specs=[IN_VMEM] * 2,
        out_shape=[
            jax.ShapeDtypeStruct(residual.shape, BF),
            jax.ShapeDtypeStruct(shape, BF),
        ],
        compiler_params=grant(16),
        name="mix",
    )(projected, residual, scale[None, :], selector)


def deal_kernel(arrived_ref, out_ref):
    total, _ = arrived_ref.shape
    count, each = total // FOLD, out_ref.shape[1]
    unfold = picking(total, total, lambda i: i % count * FOLD + i // count)
    rows = jnp.dot(unfold, arrived_ref[...], preferred_element_type=F32).astype(BF)
    for k in range(NSHARE):
        mine = jnp.concatenate(
            [rows[j * count + k * each : j * count + (k + 1) * each] for j in range(FOLD)],
            axis=1,
        )
        for i, colour in enumerate(COLOURS):
            if colour == k:
                out_ref[i] = mine


def deal(arrived):
    total, width = arrived.shape
    return pl.pallas_call(
        deal_kernel,
        in_specs=[IN_VMEM],
        out_specs=IN_VMEM,
        out_shape=jax.ShapeDtypeStruct((NT, total // FOLD // NSHARE, width * FOLD), BF),
        compiler_params=grant(16),
        name="deal",
    )(arrived)


def collect_kernel(back_ref, out_ref):
    classes = []
    for k in range(NSHARE):
        total = None
        for i, colour in enumerate(COLOURS):
            if colour == k:
                part = back_ref[i].astype(F32)
                total = part if total is None else total + part
        classes.append(total.astype(BF))
    rows = jnp.concatenate(classes, axis=0)
    count = rows.shape[0]
    fold = picking(
        FOLD * count, FOLD * count, lambda i: i % FOLD * count + i // FOLD
    )
    out_ref[...] = jnp.dot(fold, folded(rows), preferred_element_type=F32).astype(BF)


def collect(back):
    _, each, depth = back.shape
    return pl.pallas_call(
        collect_kernel,
        in_specs=[IN_VMEM],
        out_specs=IN_VMEM,
        out_shape=jax.ShapeDtypeStruct((NSHARE * each * FOLD, depth // FOLD), BF),
        compiler_params=grant(16),
        name="collect",
    )(back)


def finish_kernel(mixed_ref, returned_ref, weights_ref, *refs):
    picks, out_ref = refs[:-1], refs[-1]
    tokens, depth = mixed_ref.shape
    width = depth // FOLD
    found = [
        jnp.dot(pick[...], returned_ref[...], preferred_element_type=F32) for pick in picks
    ]
    for j in range(FOLD):
        cols, rows = slice(j * width, (j + 1) * width), slice(j * tokens, (j + 1) * tokens)
        moe = sum(f[rows] * weights_ref[:, k : k + 1] for k, f in enumerate(found))
        out_ref[:, cols] = (mixed_ref[:, cols].astype(F32) + moe).astype(BF)


def finish(mixed, returned, weights, picks):
    return pl.pallas_call(
        finish_kernel,
        in_specs=[IN_VMEM] * (3 + len(picks)),
        out_specs=IN_VMEM,
        out_shape=jax.ShapeDtypeStruct(mixed.shape, BF),
        compiler_params=grant(16),
        name="finish",
    )(mixed, returned, weights, *picks)


def pack_kernel(gate_ref, up_ref, down_ref, *out_refs):
    gate_up = jnp.concatenate([gate_ref[0].T, up_ref[0].T], axis=0)
    for half in range(2):
        @pl.when(pl.program_id(0) == half)
        def _():
            out_refs[half][...] = gate_up
            out_refs[2 + half][...] = down_ref[0]


def pack(w_gate, w_up, w_down):
    _, depth, units = w_gate.shape
    wide = pl.BlockSpec((1, depth, SHARE), lambda i: (0, 0, i))
    shapes = [(2 * SHARE, depth)] * 2 + [(SHARE, depth)] * 2
    outs = pl.pallas_call(
        pack_kernel,
        grid=(units // SHARE,),
        in_specs=[wide, wide, pl.BlockSpec((1, SHARE, depth), lambda i: (0, i, 0))],
        out_specs=[pl.BlockSpec(shape, lambda i: (0, 0)) for shape in shapes],
        out_shape=[jax.ShapeDtypeStruct(shape, BF) for shape in shapes],
        name="pack",
    )(w_gate, w_up, w_down)
    return outs[:2], outs[2:]


def experts_kernel(rows_ref, *refs):
    pieces, (out_ref, held, acc, sems) = refs[:-4], refs[-4:]
    pairs = len(pieces) // 4
    ups, downs = pieces[: 2 * pairs], pieces[2 * pairs :]
    copies = []
    for p in range(pairs):
        for j in range(3):
            for i in range(2):
                source = downs[2 * p + i]
                if j < 2:
                    source = ups[2 * p + i].at[pl.ds(j * SHARE, SHARE)]
                copies.append(
                    pltpu.make_async_copy(
                        source, held.at[p, j, pl.ds(i * SHARE, SHARE)], sems.at[p, j, i]
                    )
                )
    for copy in copies[:12]:
        copy.start()
    across = (((1,), (1,)), ((), ()))
    for p in range(pairs):
        gate_up = []
        for j in range(2):
            for copy in copies[6 * p + 2 * j : 6 * p + 2 * j + 2]:
                copy.wait()
            gate_up.append(
                lax.dot_general(
                    rows_ref[...], held[p, j], across, preferred_element_type=F32
                )
            )
        gate, upper = gate_up
        hidden = (gate / (1.0 + jnp.exp(-gate)) * upper).astype(BF)
        for copy in copies[6 * p + 4 : 6 * p + 6]:
            copy.wait()
        for copy in copies[6 * (p + 2) : 6 * (p + 3)]:
            copy.start()
        part = jnp.dot(hidden, held[p, 2], preferred_element_type=F32)
        if p == 0:
            acc[...] = part
        elif p < pairs - 1:
            acc[...] += part
        else:
            out_ref[...] = (acc[...] + part).astype(BF)


def experts(rows, pieces):
    pairs, depth = len(pieces) // 4, rows.shape[1]
    return pl.pallas_call(
        experts_kernel,
        in_specs=[IN_VMEM] + [IN_HBM] * len(pieces),
        out_specs=IN_VMEM,
        out_shape=jax.ShapeDtypeStruct(rows.shape, BF),
        scratch_shapes=[
            pltpu.VMEM((pairs, 3, 2 * SHARE, depth), BF),
            pltpu.VMEM(rows.shape, F32),
            pltpu.SemaphoreType.DMA((pairs, 3, 2)),
        ],
        compiler_params=grant(EXPERT_GRANT),
        name="experts",
    )(rows, *pieces)


def local(
    queries,
    keys,
    values,
    query_gain,
    key_gain,
    out_proj,
    expert_norm_scale,
    residual,
    routes,
    route_weights,
    w_gate,
    w_up,
    w_down,
):
    width = query_gain.shape[0]
    tok_sp = queries.shape[0]
    tok_dev, depth = residual.shape
    top = routes.shape[1]
    z, c = lax.axis_index("z"), lax.axis_index("c")
    yh, yl, x = lax.axis_index("yh"), lax.axis_index("yl"), lax.axis_index("x")
    start = (z * NC + c) * tok_sp

    q8 = prepare_queries(queries, query_gain, start)
    q8 = exchange(q8, GROUP)
    kv = prepare_keys(keys, values, key_gain, yl * NX + x, yh, start)
    q8, kv = lax.optimization_barrier((q8, kv))
    kv_mine = exchange(kv, "z").reshape(-1, 2 * width)
    kv_other = swap_cores(kv_mine)

    ups, downs = pack(w_gate, w_up, w_down)
    axes = ("x", ("yh", "yl"))
    pieces = []
    for packs in (ups, downs):
        left = [ring(p, axis, 1) for p, axis in zip(packs, axes)]
        right = [ring(p, axis, -1) for p, axis in zip(packs, axes)]
        last = [ring(p, axis, 1) for p, axis in zip(left, axes)]
        pieces += [*packs, *left, *right, *last]

    parts = attend(q8, kv_mine, kv_other)
    parts = exchange(parts, GROUP)
    attn_all = exchange(combine(parts), TP).reshape(NT * width, tok_sp)
    columns = lax.dot_general(
        attn_all, out_proj, (((0,), (0,)), ((), ())), preferred_element_type=F32
    ).astype(BF)
    projected = exchange(columns.reshape(NT, tok_dev, -1), TP)

    cap = max(2, 2 * tok_dev * top // (NZ * NC))
    tok = jnp.arange(tok_dev, dtype=jnp.int32)
    before = tok[None, :] < tok[:, None]
    place = jnp.arange(NZ * NC * cap * FOLD, dtype=jnp.int32)
    row = jnp.arange(FOLD * tok_dev, dtype=jnp.int32)
    same_fold = (row // tok_dev)[:, None] == (place % FOLD)[None, :]
    picks = []
    for k in range(top):
        mine = routes[:, k]
        slot = sum(
            jnp.sum(
                ((mine[:, None] == routes[:, j][None, :]) & before).astype(jnp.int32), axis=1
            )
            for j in range(top)
        )
        target = jnp.tile(mine * cap + slot, FOLD)
        picks.append(
            (same_fold & (target[:, None] == (place // FOLD)[None, :])).astype(BF)
        )
    mixed, sent = mix(projected, residual, expert_norm_scale, sum(picks).T)
    blocks = (NZ * NC, cap * FOLD, depth // FOLD)
    arrived = exchange(sent.reshape(blocks), ("z", "c"))

    rows = exchange(deal(arrived.reshape(sent.shape)), TP)
    partial = experts(rows.reshape(-1, depth), pieces)
    back = exchange(partial.reshape(rows.shape), TP)
    returned = exchange(collect(back).reshape(blocks), ("z", "c"))
    return finish(mixed, returned.reshape(sent.shape), route_weights, picks)


def solution(mesh):
    fine = Mesh(
        mesh.devices.reshape(NZ, NC, NYH, NYL, NX), ("z", "c", "yh", "yl", "x")
    )
    sp, both = ("z", "c"), ("z", "c", "yh", "yl", "x")
    placed = (
        P(sp, TP),
        P(sp, None),
        P(sp, None),
        P(),
        P(),
        P(None, TP),
        P(),
        P(both, None),
        P(both, None),
        P(both, None),
        P(sp, None, TP),
        P(sp, None, TP),
        P(sp, TP, None),
    )
    return jax.shard_map(
        local, mesh=fine, in_specs=placed, out_specs=P(both, None), check_vma=False
    )
```

```python
import math

import jax
import jax.numpy as jnp
from jax import lax
from jax.experimental import pallas as pl
from jax.experimental.pallas import tpu as pltpu
from jax.sharding import Mesh, PartitionSpec as P


GRID_W = 64
EPS = 1e-06
ROPE_BASE = 10000.0
LOG2E = 1.4426950408889634
BF = jnp.bfloat16
F32 = jnp.float32

NZ, NC, NYH, NYL, NX = 16, 2, 2, 2, 4
NY = NYH * NYL
NT = NY * NX
NG = NYL * NX
TP = ("yh", "yl", "x")
GROUP = ("yl", "x")
STAT_ROWS = 16
FOLD = 8
EXPERT_GRANT = 46
SHARE = 128
NSHARE = 4
COLOURS = tuple((i % NX + i // NX) % NSHARE for i in range(NT))


IN_VMEM = pl.BlockSpec(memory_space=pltpu.VMEM)
IN_HBM = pl.BlockSpec(memory_space=pltpu.HBM)


def grant(mib):
    return pltpu.CompilerParams(vmem_limit_bytes=mib * 1024 * 1024)


def exchange(blocks, axis):
    return lax.all_to_all(blocks, axis, split_axis=0, concat_axis=0, tiled=True)


def swap_cores(value):
    return lax.ppermute(value, "c", [(0, 1), (1, 0)])


def ring(value, axis, step):
    return lax.ppermute(value, axis, [(i, (i + step) % 4) for i in range(4)])


def turned(field, gain, start):
    count, width = field.shape
    quarter = width // 4
    f = field.astype(F32)
    f = f * lax.rsqrt(jnp.mean(f * f, axis=-1, keepdims=True) + EPS) * gain
    lane = lax.broadcasted_iota(jnp.int32, (count, width), 1)
    position = start + lax.broadcasted_iota(jnp.int32, (count, width), 0)
    coord = jnp.where(lane < 2 * quarter, position // GRID_W, position % GRID_W)
    step = (lane % quarter).astype(F32) / quarter
    angle = coord.astype(F32) * jnp.exp(step * (-math.log(ROPE_BASE)))
    first = lane % (2 * quarter) < quarter
    ahead = pltpu.roll(f, width - quarter, 1)
    behind = pltpu.roll(f, quarter, 1)
    other = jnp.where(first, -ahead, behind)
    return (f * jnp.cos(angle) + other * jnp.sin(angle)).astype(BF)


def queries_kernel(start_ref, q_ref, gain_ref, out_ref):
    q_rot = turned(q_ref[...], gain_ref[...], start_ref[0])
    for i in range(out_ref.shape[0]):
        out_ref[i] = q_rot


def prepare_queries(queries, gain, start):
    return pl.pallas_call(
        queries_kernel,
        in_specs=[pl.BlockSpec(memory_space=pltpu.SMEM), IN_VMEM, IN_VMEM],
        out_specs=IN_VMEM,
        out_shape=jax.ShapeDtypeStruct((NG, *queries.shape), BF),
        name="prepare_queries",
    )(start.reshape(1), queries, gain[None, :])


def keys_kernel(at_ref, k_ref, v_ref, gain_ref, out_ref):
    k_rot = turned(k_ref[...], gain_ref[...], at_ref[2])
    both = jnp.concatenate([k_rot, v_ref[...]], axis=1)
    for i in range(out_ref.shape[0]):
        out_ref[i] = both


def prepare_keys(keys, values, gain, block, head, start):
    width = gain.shape[0]
    size = keys.shape[0] // NG
    at = jnp.stack([block, head, start + block * size]).astype(jnp.int32)
    part = pl.BlockSpec((size, width), lambda i, at: (at[0], at[1]))
    out = (NZ, size, 2 * width)
    return pl.pallas_call(
        keys_kernel,
        grid_spec=pltpu.PrefetchScalarGridSpec(
            num_scalar_prefetch=1,
            grid=(1,),
            in_specs=[part, part, pl.BlockSpec((1, width), lambda i, at: (0, 0))],
            out_specs=pl.BlockSpec(out, lambda i, at: (0, 0, 0)),
        ),
        out_shape=jax.ShapeDtypeStruct(out, BF),
        name="prepare_keys",
    )(at, keys, values, gain[None, :])


def split3(x):
    hi = x.astype(BF)
    rest = x - hi.astype(F32)
    mid = rest.astype(BF)
    lo = (rest - mid.astype(F32)).astype(BF)
    return hi, mid, lo


def attend_kernel(q_ref, own_ref, other_ref, out_ref, scores_ref):
    heads, rows, width = q_ref.shape
    factor = width ** (-0.5) * LOG2E
    keys = jnp.concatenate([own_ref[:, :width], other_ref[:, :width]], axis=0)
    values = jnp.concatenate([own_ref[:, width:], other_ref[:, width:]], axis=0)
    values = jnp.concatenate(
        [values.T, jnp.ones((STAT_ROWS, values.shape[0]), BF)], axis=0
    )
    row = lax.broadcasted_iota(jnp.int32, (STAT_ROWS, rows), 0)

    def score(head):
        scores_ref[head % 2] = lax.dot_general(
            keys, q_ref[head], (((1,), (1,)), ((), ())), preferred_element_type=F32
        )

    score(0)
    for head in range(heads):
        if head + 1 < heads:
            score(head + 1)
        scores = scores_ref[head % 2]
        top = jnp.max(scores, axis=0, keepdims=True)
        weights = jnp.exp2((scores - top) * factor).astype(BF)
        summed = jnp.dot(values, weights, preferred_element_type=F32)
        total = summed[width : width + 1]
        out_ref[head, :width, :] = (summed[:width] * (1.0 / total)).astype(BF)
        stats = jnp.zeros((STAT_ROWS, rows), F32)
        for i, part in enumerate(split3(top * factor) + split3(total)):
            stats = jnp.where(row == i, part.astype(F32), stats)
        out_ref[head, width:, :] = stats.astype(BF)


def attend(q8, own, other):
    heads, rows, width = q8.shape
    return pl.pallas_call(
        attend_kernel,
        in_specs=[IN_VMEM] * 3,
        out_specs=IN_VMEM,
        out_shape=jax.ShapeDtypeStruct((heads, width + STAT_ROWS, rows), BF),
        scratch_shapes=[pltpu.VMEM((2, NC * own.shape[0], rows), F32)],
        compiler_params=grant(24),
        name="attend",
    )(q8, own, other)


def combine_kernel(parts_ref, out_ref):
    count = parts_ref.shape[0]
    width = out_ref.shape[1]
    tops, totals = [], []
    for j in range(count):
        s = parts_ref[j, width:, :].astype(F32)
        tops.append(s[0:1] + s[1:2] + s[2:3])
        totals.append(s[3:4] + s[4:5] + s[5:6])
    top = tops[0]
    for j in range(1, count):
        top = jnp.maximum(top, tops[j])
    shares = [totals[j] * jnp.exp2(tops[j] - top) for j in range(count)]
    whole = sum(shares[1:], shares[0])
    acc = jnp.zeros(out_ref.shape[1:], F32)
    for j in range(count):
        acc = acc + parts_ref[j, :width, :].astype(F32) * (shares[j] / whole)
    done = acc.astype(BF)
    for i in range(out_ref.shape[0]):
        out_ref[i] = done


def combine(parts):
    width = parts.shape[1] - STAT_ROWS
    return pl.pallas_call(
        combine_kernel,
        in_specs=[IN_VMEM],
        out_specs=IN_VMEM,
        out_shape=jax.ShapeDtypeStruct((NT, width, parts.shape[2]), BF),
        compiler_params=grant(16),
        name="combine",
    )(parts)


def folded(rows):
    width = rows.shape[1] // FOLD
    return jnp.concatenate(
        [rows[:, j * width : (j + 1) * width] for j in range(FOLD)], axis=0
    )


def picking(outs, ins, source_of):
    i = lax.broadcasted_iota(jnp.int32, (outs, ins), 0)
    r = lax.broadcasted_iota(jnp.int32, (outs, ins), 1)
    return jnp.where(r == source_of(i), 1.0, 0.0).astype(BF)


def mix_kernel(projected_ref, residual_ref, scale_ref, selector_ref, mixed_ref, sent_ref):
    projected = jnp.concatenate(
        [projected_ref[i].astype(F32) for i in range(projected_ref.shape[0])], axis=1
    )
    mixed = (residual_ref[...].astype(F32) + projected).astype(BF)
    mixed_ref[...] = mixed
    mixed = mixed.astype(F32)
    mean = jnp.mean(mixed * mixed, axis=-1, keepdims=True)
    normed = (mixed * lax.rsqrt(mean + EPS) * scale_ref[...]).astype(BF)
    sent_ref[...] = jnp.dot(
        selector_ref[...], folded(normed), preferred_element_type=F32
    ).astype(BF)


def mix(projected, residual, scale, selector):
    shape = (selector.shape[0], residual.shape[1] // FOLD)
    return pl.pallas_call(
        mix_kernel,
        in_specs=[IN_VMEM] * 4,
        out_specs=[IN_VMEM] * 2,
        out_shape=[
            jax.ShapeDtypeStruct(residual.shape, BF),
            jax.ShapeDtypeStruct(shape, BF),
        ],
        compiler_params=grant(16),
        name="mix",
    )(projected, residual, scale[None, :], selector)


def deal_kernel(arrived_ref, out_ref):
    total, _ = arrived_ref.shape
    count, each = total // FOLD, out_ref.shape[1]
    unfold = picking(total, total, lambda i: i % count * FOLD + i // count)
    rows = jnp.dot(unfold, arrived_ref[...], preferred_element_type=F32).astype(BF)
    for k in range(NSHARE):
        mine = jnp.concatenate(
            [rows[j * count + k * each : j * count + (k + 1) * each] for j in range(FOLD)],
            axis=1,
        )
        for i, colour in enumerate(COLOURS):
            if colour == k:
                out_ref[i] = mine


def deal(arrived):
    total, width = arrived.shape
    return pl.pallas_call(
        deal_kernel,
        in_specs=[IN_VMEM],
        out_specs=IN_VMEM,
        out_shape=jax.ShapeDtypeStruct((NT, total // FOLD // NSHARE, width * FOLD), BF),
        compiler_params=grant(16),
        name="deal",
    )(arrived)


def collect_kernel(back_ref, out_ref):
    classes = []
    for k in range(NSHARE):
        total = None
        for i, colour in enumerate(COLOURS):
            if colour == k:
                part = back_ref[i].astype(F32)
                total = part if total is None else total + part
        classes.append(total.astype(BF))
    rows = jnp.concatenate(classes, axis=0)
    count = rows.shape[0]
    fold = picking(
        FOLD * count, FOLD * count, lambda i: i % FOLD * count + i // FOLD
    )
    out_ref[...] = jnp.dot(fold, folded(rows), preferred_element_type=F32).astype(BF)


def collect(back):
    _, each, depth = back.shape
    return pl.pallas_call(
        collect_kernel,
        in_specs=[IN_VMEM],
        out_specs=IN_VMEM,
        out_shape=jax.ShapeDtypeStruct((NSHARE * each * FOLD, depth // FOLD), BF),
        compiler_params=grant(16),
        name="collect",
    )(back)


def finish_kernel(mixed_ref, returned_ref, weights_ref, *refs):
    picks, out_ref = refs[:-1], refs[-1]
    tokens, depth = mixed_ref.shape
    width = depth // FOLD
    found = [
        jnp.dot(pick[...], returned_ref[...], preferred_element_type=F32) for pick in picks
    ]
    for j in range(FOLD):
        cols, rows = slice(j * width, (j + 1) * width), slice(j * tokens, (j + 1) * tokens)
        moe = sum(f[rows] * weights_ref[:, k : k + 1] for k, f in enumerate(found))
        out_ref[:, cols] = (mixed_ref[:, cols].astype(F32) + moe).astype(BF)


def finish(mixed, returned, weights, picks):
    return pl.pallas_call(
        finish_kernel,
        in_specs=[IN_VMEM] * (3 + len(picks)),
        out_specs=IN_VMEM,
        out_shape=jax.ShapeDtypeStruct(mixed.shape, BF),
        compiler_params=grant(16),
        name="finish",
    )(mixed, returned, weights, *picks)


def pack_kernel(gate_ref, up_ref, down_ref, *out_refs):
    gate_up = jnp.concatenate([gate_ref[0].T, up_ref[0].T], axis=0)
    for half in range(2):
        @pl.when(pl.program_id(0) == half)
        def _():
            out_refs[half][...] = gate_up
            out_refs[2 + half][...] = down_ref[0]


def pack(w_gate, w_up, w_down):
    _, depth, units = w_gate.shape
    wide = pl.BlockSpec((1, depth, SHARE), lambda i: (0, 0, i))
    shapes = [(2 * SHARE, depth)] * 2 + [(SHARE, depth)] * 2
    outs = pl.pallas_call(
        pack_kernel,
        grid=(units // SHARE,),
        in_specs=[wide, wide, pl.BlockSpec((1, SHARE, depth), lambda i: (0, i, 0))],
        out_specs=[pl.BlockSpec(shape, lambda i: (0, 0)) for shape in shapes],
        out_shape=[jax.ShapeDtypeStruct(shape, BF) for shape in shapes],
        name="pack",
    )(w_gate, w_up, w_down)
    return outs[:2], outs[2:]


def experts_kernel(rows_ref, own_up_ref, own_down_ref, *refs):
    pieces, (out_ref, held, acc, sems) = refs[:-4], refs[-4:]
    count = len(pieces) // 2
    ups, downs = pieces[:count], pieces[count:]
    pairs = (count + 1) // 2
    copies = [[[] for _ in range(3)] for _ in range(pairs)]
    for n in range(count):
        p, i = (n + 1) // 2, (n + 1) % 2
        for j in range(3):
            source = downs[n] if j == 2 else ups[n].at[pl.ds(j * SHARE, SHARE)]
            copies[p][j].append(
                pltpu.make_async_copy(
                    source, held.at[p, j, pl.ds(i * SHARE, SHARE)], sems.at[p, j, i]
                )
            )

    def start(p):
        for group in copies[p] if p < pairs else []:
            for copy in group:
                copy.start()

    def wait(p, j):
        for copy in copies[p][j]:
            copy.wait()

    def against(units):
        return lax.dot_general(
            rows_ref[...], units, (((1,), (1,)), ((), ())), preferred_element_type=F32
        )

    def swish(gate, upper):
        return (gate / (1.0 + jnp.exp(-gate)) * upper).astype(BF)

    start(0)
    start(1)
    both = against(own_up_ref[...])
    mine = swish(both[:, :SHARE], both[:, SHARE:])
    wait(0, 0)
    wait(0, 1)
    gate = against(held[0, 0, SHARE:])
    hidden = jnp.concatenate([mine, swish(gate, against(held[0, 1, SHARE:]))], axis=1)
    wait(0, 2)
    start(2)
    down = jnp.concatenate([own_down_ref[...], held[0, 2, SHARE:]], axis=0)
    acc[...] = jnp.dot(hidden, down, preferred_element_type=F32)
    for p in range(1, pairs):
        wait(p, 0)
        gate = against(held[p, 0])
        wait(p, 1)
        hidden = swish(gate, against(held[p, 1]))
        wait(p, 2)
        start(p + 2)
        part = jnp.dot(hidden, held[p, 2], preferred_element_type=F32)
        if p < pairs - 1:
            acc[...] += part
        else:
            out_ref[...] = (acc[...] + part).astype(BF)


def experts(rows, ups, downs):
    pairs, depth = len(ups) // 2, rows.shape[1]
    pieces = [*ups[1:], *downs[1:]]
    return pl.pallas_call(
        experts_kernel,
        in_specs=[IN_VMEM] * 3 + [IN_HBM] * len(pieces),
        out_specs=IN_VMEM,
        out_shape=jax.ShapeDtypeStruct(rows.shape, BF),
        scratch_shapes=[
            pltpu.VMEM((pairs, 3, 2 * SHARE, depth), BF),
            pltpu.VMEM(rows.shape, F32),
            pltpu.SemaphoreType.DMA((pairs, 3, 2)),
        ],
        compiler_params=grant(EXPERT_GRANT),
        name="experts",
    )(rows, ups[0], downs[0], *pieces)


def local(
    queries,
    keys,
    values,
    query_gain,
    key_gain,
    out_proj,
    expert_norm_scale,
    residual,
    routes,
    route_weights,
    w_gate,
    w_up,
    w_down,
):
    width = query_gain.shape[0]
    tok_sp = queries.shape[0]
    tok_dev, depth = residual.shape
    top = routes.shape[1]
    z, c = lax.axis_index("z"), lax.axis_index("c")
    yh, yl, x = lax.axis_index("yh"), lax.axis_index("yl"), lax.axis_index("x")
    start = (z * NC + c) * tok_sp

    q8 = prepare_queries(queries, query_gain, start)
    q8 = exchange(q8, GROUP)
    kv = prepare_keys(keys, values, key_gain, yl * NX + x, yh, start)
    q8, kv = lax.optimization_barrier((q8, kv))
    kv_mine = exchange(kv, "z").reshape(-1, 2 * width)
    kv_other = swap_cores(kv_mine)

    ups, downs = pack(w_gate, w_up, w_down)
    axes = ("x", ("yh", "yl"))
    pieces = []
    for packs in (ups, downs):
        left = [ring(p, axis, 1) for p, axis in zip(packs, axes)]
        right = [ring(p, axis, -1) for p, axis in zip(packs, axes)]
        last = [ring(p, axis, 1) for p, axis in zip(left, axes)]
        pieces.append([*packs, *left, *right, *last])

    parts = attend(q8, kv_mine, kv_other)
    parts = exchange(parts, GROUP)
    attn_all = exchange(combine(parts), TP).reshape(NT * width, tok_sp)
    columns = lax.dot_general(
        attn_all, out_proj, (((0,), (0,)), ((), ())), preferred_element_type=F32
    ).astype(BF)
    projected = exchange(columns.reshape(NT, tok_dev, -1), TP)

    cap = max(2, 2 * tok_dev * top // (NZ * NC))
    tok = jnp.arange(tok_dev, dtype=jnp.int32)
    before = tok[None, :] < tok[:, None]
    place = jnp.arange(NZ * NC * cap * FOLD, dtype=jnp.int32)
    row = jnp.arange(FOLD * tok_dev, dtype=jnp.int32)
    same_fold = (row // tok_dev)[:, None] == (place % FOLD)[None, :]
    picks = []
    for k in range(top):
        mine = routes[:, k]
        slot = sum(
            jnp.sum(
                ((mine[:, None] == routes[:, j][None, :]) & before).astype(jnp.int32), axis=1
            )
            for j in range(top)
        )
        target = jnp.tile(mine * cap + slot, FOLD)
        picks.append(
            (same_fold & (target[:, None] == (place // FOLD)[None, :])).astype(BF)
        )
    mixed, sent = mix(projected, residual, expert_norm_scale, sum(picks).T)
    blocks = (NZ * NC, cap * FOLD, depth // FOLD)
    arrived = exchange(sent.reshape(blocks), ("z", "c"))

    rows = exchange(deal(arrived.reshape(sent.shape)), TP)
    partial = experts(rows.reshape(-1, depth), *pieces)
    back = exchange(partial.reshape(rows.shape), TP)
    returned = exchange(collect(back).reshape(blocks), ("z", "c"))
    return finish(mixed, returned.reshape(sent.shape), route_weights, picks)


def solution(mesh):
    fine = Mesh(
        mesh.devices.reshape(NZ, NC, NYH, NYL, NX), ("z", "c", "yh", "yl", "x")
    )
    sp, both = ("z", "c"), ("z", "c", "yh", "yl", "x")
    placed = (
        P(sp, TP),
        P(sp, None),
        P(sp, None),
        P(),
        P(),
        P(None, TP),
        P(),
        P(both, None),
        P(both, None),
        P(both, None),
        P(sp, None, TP),
        P(sp, None, TP),
        P(sp, TP, None),
    )
    return jax.shard_map(
        local, mesh=fine, in_specs=placed, out_specs=P(both, None), check_vma=False
    )
```

```python
import math

import jax
import jax.numpy as jnp
from jax import lax
from jax.experimental import pallas as pl
from jax.experimental.pallas import tpu as pltpu
from jax.sharding import Mesh, PartitionSpec as P


GRID_W = 64
EPS = 1e-06
ROPE_BASE = 10000.0
LOG2E = 1.4426950408889634
BF = jnp.bfloat16
F32 = jnp.float32

NZ, NC, NYH, NYL, NX = 16, 2, 2, 2, 4
NY = NYH * NYL
NT = NY * NX
NG = NYL * NX
TP = ("yh", "yl", "x")
GROUP = ("yl", "x")
STAT_ROWS = 16
FOLD = 8
EXPERT_GRANT = 46
SHARE = 128
NSHARE = 4
COLOURS = tuple((i % NX + i // NX) % NSHARE for i in range(NT))


IN_VMEM = pl.BlockSpec(memory_space=pltpu.VMEM)
IN_HBM = pl.BlockSpec(memory_space=pltpu.HBM)


def grant(mib):
    return pltpu.CompilerParams(vmem_limit_bytes=mib * 1024 * 1024)


def exchange(blocks, axis):
    return lax.all_to_all(blocks, axis, split_axis=0, concat_axis=0, tiled=True)


def swap_cores(value):
    return lax.ppermute(value, "c", [(0, 1), (1, 0)])


def ring(value, axis, step):
    return lax.ppermute(value, axis, [(i, (i + step) % 4) for i in range(4)])


def turned(field, gain, start):
    count, width = field.shape
    quarter = width // 4
    f = field.astype(F32)
    f = f * lax.rsqrt(jnp.mean(f * f, axis=-1, keepdims=True) + EPS) * gain
    lane = lax.broadcasted_iota(jnp.int32, (count, width), 1)
    position = start + lax.broadcasted_iota(jnp.int32, (count, width), 0)
    coord = jnp.where(lane < 2 * quarter, position // GRID_W, position % GRID_W)
    step = (lane % quarter).astype(F32) / quarter
    angle = coord.astype(F32) * jnp.exp(step * (-math.log(ROPE_BASE)))
    first = lane % (2 * quarter) < quarter
    ahead = pltpu.roll(f, width - quarter, 1)
    behind = pltpu.roll(f, quarter, 1)
    other = jnp.where(first, -ahead, behind)
    return (f * jnp.cos(angle) + other * jnp.sin(angle)).astype(BF)


def queries_kernel(start_ref, q_ref, gain_ref, out_ref):
    q_rot = turned(q_ref[...], gain_ref[...], start_ref[0])
    for i in range(out_ref.shape[0]):
        out_ref[i] = q_rot


def prepare_queries(queries, gain, start):
    return pl.pallas_call(
        queries_kernel,
        in_specs=[pl.BlockSpec(memory_space=pltpu.SMEM), IN_VMEM, IN_VMEM],
        out_specs=IN_VMEM,
        out_shape=jax.ShapeDtypeStruct((NG, *queries.shape), BF),
        name="prepare_queries",
    )(start.reshape(1), queries, gain[None, :])


def keys_kernel(at_ref, k_ref, v_ref, gain_ref, out_ref):
    k_rot = turned(k_ref[...], gain_ref[...], at_ref[2])
    both = jnp.concatenate([k_rot, v_ref[...]], axis=1)
    for i in range(out_ref.shape[0]):
        out_ref[i] = both


def prepare_keys(keys, values, gain, block, head, start):
    width = gain.shape[0]
    size = keys.shape[0] // NG
    at = jnp.stack([block, head, start + block * size]).astype(jnp.int32)
    part = pl.BlockSpec((size, width), lambda i, at: (at[0], at[1]))
    out = (NZ, size, 2 * width)
    return pl.pallas_call(
        keys_kernel,
        grid_spec=pltpu.PrefetchScalarGridSpec(
            num_scalar_prefetch=1,
            grid=(1,),
            in_specs=[part, part, pl.BlockSpec((1, width), lambda i, at: (0, 0))],
            out_specs=pl.BlockSpec(out, lambda i, at: (0, 0, 0)),
        ),
        out_shape=jax.ShapeDtypeStruct(out, BF),
        name="prepare_keys",
    )(at, keys, values, gain[None, :])


def split3(x):
    hi = x.astype(BF)
    rest = x - hi.astype(F32)
    mid = rest.astype(BF)
    lo = (rest - mid.astype(F32)).astype(BF)
    return hi, mid, lo


def attend_kernel(q_ref, own_ref, other_ref, out_ref, scores_ref):
    heads, rows, width = q_ref.shape
    factor = width ** (-0.5) * LOG2E
    keys = jnp.concatenate([own_ref[:, :width], other_ref[:, :width]], axis=0)
    values = jnp.concatenate([own_ref[:, width:], other_ref[:, width:]], axis=0)
    values = jnp.concatenate(
        [values.T, jnp.ones((STAT_ROWS, values.shape[0]), BF)], axis=0
    )
    row = lax.broadcasted_iota(jnp.int32, (STAT_ROWS, rows), 0)

    def score(head):
        scores_ref[head % 2] = lax.dot_general(
            keys, q_ref[head], (((1,), (1,)), ((), ())), preferred_element_type=F32
        )

    score(0)
    for head in range(heads):
        if head + 1 < heads:
            score(head + 1)
        scores = scores_ref[head % 2]
        top = jnp.max(scores, axis=0, keepdims=True)
        weights = jnp.exp2((scores - top) * factor).astype(BF)
        summed = jnp.dot(values, weights, preferred_element_type=F32)
        total = summed[width : width + 1]
        out_ref[head, :width, :] = (summed[:width] * (1.0 / total)).astype(BF)
        stats = jnp.zeros((STAT_ROWS, rows), F32)
        for i, part in enumerate(split3(top * factor) + split3(total)):
            stats = jnp.where(row == i, part.astype(F32), stats)
        out_ref[head, width:, :] = stats.astype(BF)


def attend(q8, own, other):
    heads, rows, width = q8.shape
    return pl.pallas_call(
        attend_kernel,
        in_specs=[IN_VMEM] * 3,
        out_specs=IN_VMEM,
        out_shape=jax.ShapeDtypeStruct((heads, width + STAT_ROWS, rows), BF),
        scratch_shapes=[pltpu.VMEM((2, NC * own.shape[0], rows), F32)],
        compiler_params=grant(24),
        name="attend",
    )(q8, own, other)


def combine_kernel(parts_ref, out_ref):
    count = parts_ref.shape[0]
    width = out_ref.shape[1]
    tops, totals = [], []
    for j in range(count):
        s = parts_ref[j, width:, :].astype(F32)
        tops.append(s[0:1] + s[1:2] + s[2:3])
        totals.append(s[3:4] + s[4:5] + s[5:6])
    top = tops[0]
    for j in range(1, count):
        top = jnp.maximum(top, tops[j])
    shares = [totals[j] * jnp.exp2(tops[j] - top) for j in range(count)]
    whole = sum(shares[1:], shares[0])
    acc = jnp.zeros((width, parts_ref.shape[2]), F32)
    for j in range(count):
        acc = acc + parts_ref[j, :width, :].astype(F32) * (shares[j] / whole)
    done = acc.astype(BF)
    part = done.shape[1] // (NYH * NYL)
    halves = [
        jnp.concatenate(
            [
                done[:, (NYL * i + k) * part : (NYL * i + k + 1) * part]
                for i in range(NYH)
            ],
            axis=1,
        )
        for k in range(NYL)
    ]
    for i in range(out_ref.shape[0]):
        out_ref[i] = halves[i // NX % NYL]


def combine(parts):
    width = parts.shape[1] - STAT_ROWS
    return pl.pallas_call(
        combine_kernel,
        in_specs=[IN_VMEM],
        out_specs=IN_VMEM,
        out_shape=jax.ShapeDtypeStruct((NT, width, parts.shape[2] // NYL), BF),
        compiler_params=grant(16),
        name="combine",
    )(parts)


def folded(rows):
    width = rows.shape[1] // FOLD
    return jnp.concatenate(
        [rows[:, j * width : (j + 1) * width] for j in range(FOLD)], axis=0
    )


def picking(outs, ins, source_of):
    i = lax.broadcasted_iota(jnp.int32, (outs, ins), 0)
    r = lax.broadcasted_iota(jnp.int32, (outs, ins), 1)
    return jnp.where(r == source_of(i), 1.0, 0.0).astype(BF)


def mix_kernel(projected_ref, residual_ref, scale_ref, selector_ref, mixed_ref, sent_ref):
    width = projected_ref.shape[2] // NYL
    projected = jnp.concatenate(
        [
            projected_ref[NX * h + i, :, k * width : (k + 1) * width].astype(F32)
            for h in range(NYH)
            for k in range(NYL)
            for i in range(NX)
        ],
        axis=1,
    )
    mixed = (residual_ref[...].astype(F32) + projected).astype(BF)
    mixed_ref[...] = mixed
    mixed = mixed.astype(F32)
    mean = jnp.mean(mixed * mixed, axis=-1, keepdims=True)
    normed = (mixed * lax.rsqrt(mean + EPS) * scale_ref[...]).astype(BF)
    sent_ref[...] = jnp.dot(
        selector_ref[...], folded(normed), preferred_element_type=F32
    ).astype(BF)


def mix(projected, residual, scale, selector):
    shape = (selector.shape[0], residual.shape[1] // FOLD)
    return pl.pallas_call(
        mix_kernel,
        in_specs=[IN_VMEM] * 4,
        out_specs=[IN_VMEM] * 2,
        out_shape=[
            jax.ShapeDtypeStruct(residual.shape, BF),
            jax.ShapeDtypeStruct(shape, BF),
        ],
        compiler_params=grant(16),
        name="mix",
    )(projected, residual, scale[None, :], selector)


def deal_kernel(arrived_ref, out_ref):
    total, _ = arrived_ref.shape
    count, each = total // FOLD, out_ref.shape[1]
    unfold = picking(total, total, lambda i: i % count * FOLD + i // count)
    rows = jnp.dot(unfold, arrived_ref[...], preferred_element_type=F32).astype(BF)
    for k in range(NSHARE):
        mine = jnp.concatenate(
            [rows[j * count + k * each : j * count + (k + 1) * each] for j in range(FOLD)],
            axis=1,
        )
        for i, colour in enumerate(COLOURS):
            if colour == k:
                out_ref[i] = mine


def deal(arrived):
    total, width = arrived.shape
    return pl.pallas_call(
        deal_kernel,
        in_specs=[IN_VMEM],
        out_specs=IN_VMEM,
        out_shape=jax.ShapeDtypeStruct((NT, total // FOLD // NSHARE, width * FOLD), BF),
        compiler_params=grant(16),
        name="deal",
    )(arrived)


def collect_kernel(back_ref, out_ref):
    classes = []
    for k in range(NSHARE):
        total = None
        for i, colour in enumerate(COLOURS):
            if colour == k:
                part = back_ref[i].astype(F32)
                total = part if total is None else total + part
        classes.append(total.astype(BF))
    rows = jnp.concatenate(classes, axis=0)
    count = rows.shape[0]
    fold = picking(
        FOLD * count, FOLD * count, lambda i: i % FOLD * count + i // FOLD
    )
    out_ref[...] = jnp.dot(fold, folded(rows), preferred_element_type=F32).astype(BF)


def collect(back):
    _, each, depth = back.shape
    return pl.pallas_call(
        collect_kernel,
        in_specs=[IN_VMEM],
        out_specs=IN_VMEM,
        out_shape=jax.ShapeDtypeStruct((NSHARE * each * FOLD, depth // FOLD), BF),
        compiler_params=grant(16),
        name="collect",
    )(back)


def finish_kernel(mixed_ref, returned_ref, weights_ref, *refs):
    picks, out_ref = refs[:-1], refs[-1]
    tokens, depth = mixed_ref.shape
    width = depth // FOLD
    found = [
        jnp.dot(pick[...], returned_ref[...], preferred_element_type=F32) for pick in picks
    ]
    for j in range(FOLD):
        cols, rows = slice(j * width, (j + 1) * width), slice(j * tokens, (j + 1) * tokens)
        moe = sum(f[rows] * weights_ref[:, k : k + 1] for k, f in enumerate(found))
        out_ref[:, cols] = (mixed_ref[:, cols].astype(F32) + moe).astype(BF)


def finish(mixed, returned, weights, picks):
    return pl.pallas_call(
        finish_kernel,
        in_specs=[IN_VMEM] * (3 + len(picks)),
        out_specs=IN_VMEM,
        out_shape=jax.ShapeDtypeStruct(mixed.shape, BF),
        compiler_params=grant(16),
        name="finish",
    )(mixed, returned, weights, *picks)


def pack_kernel(gate_ref, up_ref, down_ref, *out_refs):
    gate_up = jnp.concatenate([gate_ref[0].T, up_ref[0].T], axis=0)
    for half in range(2):
        @pl.when(pl.program_id(0) == half)
        def _():
            out_refs[half][...] = gate_up
            out_refs[2 + half][...] = down_ref[0]


def pack(w_gate, w_up, w_down):
    _, depth, units = w_gate.shape
    wide = pl.BlockSpec((1, depth, SHARE), lambda i: (0, 0, i))
    shapes = [(2 * SHARE, depth)] * 2 + [(SHARE, depth)] * 2
    outs = pl.pallas_call(
        pack_kernel,
        grid=(units // SHARE,),
        in_specs=[wide, wide, pl.BlockSpec((1, SHARE, depth), lambda i: (0, i, 0))],
        out_specs=[pl.BlockSpec(shape, lambda i: (0, 0)) for shape in shapes],
        out_shape=[jax.ShapeDtypeStruct(shape, BF) for shape in shapes],
        name="pack",
    )(w_gate, w_up, w_down)
    return outs[:2], outs[2:]


def experts_kernel(rows_ref, *refs):
    pieces, (out_ref, held, acc, sems) = refs[:-4], refs[-4:]
    pairs = len(pieces) // 4
    ups, downs = pieces[: 2 * pairs], pieces[2 * pairs :]
    copies = []
    for p in range(pairs):
        for j in range(3):
            for i in range(2):
                source = downs[2 * p + i]
                if j < 2:
                    source = ups[2 * p + i].at[pl.ds(j * SHARE, SHARE)]
                copies.append(
                    pltpu.make_async_copy(
                        source, held.at[p, j, pl.ds(i * SHARE, SHARE)], sems.at[p, j, i]
                    )
                )
    for copy in copies[:12]:
        copy.start()
    across = (((1,), (1,)), ((), ()))
    for p in range(pairs):
        gate_up = []
        for j in range(2):
            for copy in copies[6 * p + 2 * j : 6 * p + 2 * j + 2]:
                copy.wait()
            gate_up.append(
                lax.dot_general(
                    rows_ref[...], held[p, j], across, preferred_element_type=F32
                )
            )
        gate, upper = gate_up
        hidden = (gate / (1.0 + jnp.exp(-gate)) * upper).astype(BF)
        for copy in copies[6 * p + 4 : 6 * p + 6]:
            copy.wait()
        for copy in copies[6 * (p + 2) : 6 * (p + 3)]:
            copy.start()
        part = jnp.dot(hidden, held[p, 2], preferred_element_type=F32)
        if p == 0:
            acc[...] = part
        elif p < pairs - 1:
            acc[...] += part
        else:
            out_ref[...] = (acc[...] + part).astype(BF)


def experts(rows, pieces):
    pairs, depth = len(pieces) // 4, rows.shape[1]
    return pl.pallas_call(
        experts_kernel,
        in_specs=[IN_VMEM] + [IN_HBM] * len(pieces),
        out_specs=IN_VMEM,
        out_shape=jax.ShapeDtypeStruct(rows.shape, BF),
        scratch_shapes=[
            pltpu.VMEM((pairs, 3, 2 * SHARE, depth), BF),
            pltpu.VMEM(rows.shape, F32),
            pltpu.SemaphoreType.DMA((pairs, 3, 2)),
        ],
        compiler_params=grant(EXPERT_GRANT),
        name="experts",
    )(rows, *pieces)


def local(
    queries,
    keys,
    values,
    query_gain,
    key_gain,
    out_proj,
    expert_norm_scale,
    residual,
    routes,
    route_weights,
    w_gate,
    w_up,
    w_down,
):
    width = query_gain.shape[0]
    tok_sp = queries.shape[0]
    tok_dev, depth = residual.shape
    top = routes.shape[1]
    z, c = lax.axis_index("z"), lax.axis_index("c")
    yh, yl, x = lax.axis_index("yh"), lax.axis_index("yl"), lax.axis_index("x")
    start = (z * NC + c) * tok_sp

    q8 = prepare_queries(queries, query_gain, start)
    q8 = exchange(q8, GROUP)
    out_proj_other = lax.ppermute(out_proj, "yl", [(0, 1), (1, 0)])
    kv = prepare_keys(keys, values, key_gain, yl * NX + x, yh, start)
    q8, kv = lax.optimization_barrier((q8, kv))
    kv_mine = exchange(kv, "z").reshape(-1, 2 * width)
    kv_other = swap_cores(kv_mine)

    ups, downs = pack(w_gate, w_up, w_down)
    axes = ("x", ("yh", "yl"))
    pieces = []
    for packs in (ups, downs):
        left = [ring(p, axis, 1) for p, axis in zip(packs, axes)]
        right = [ring(p, axis, -1) for p, axis in zip(packs, axes)]
        last = [ring(p, axis, 1) for p, axis in zip(left, axes)]
        pieces += [*packs, *left, *right, *last]

    parts = attend(q8, kv_mine, kv_other)
    parts = exchange(parts, GROUP)
    attn_all = exchange(combine(parts), TP).reshape(NT * width, -1)

    def project(columns):
        return lax.dot_general(
            attn_all, columns, (((0,), (0,)), ((), ())), preferred_element_type=F32
        ).astype(BF)

    mine, other = project(out_proj), project(out_proj_other)
    columns = jnp.concatenate(
        [jnp.where(yl == 0, mine, other), jnp.where(yl == 0, other, mine)], axis=1
    )
    projected = exchange(columns.reshape(NYH * NX, tok_dev, -1), ("yh", "x"))

    cap = max(2, 2 * tok_dev * top // (NZ * NC))
    tok = jnp.arange(tok_dev, dtype=jnp.int32)
    before = tok[None, :] < tok[:, None]
    place = jnp.arange(NZ * NC * cap * FOLD, dtype=jnp.int32)
    row = jnp.arange(FOLD * tok_dev, dtype=jnp.int32)
    same_fold = (row // tok_dev)[:, None] == (place % FOLD)[None, :]
    picks = []
    for k in range(top):
        mine = routes[:, k]
        slot = sum(
            jnp.sum(
                ((mine[:, None] == routes[:, j][None, :]) & before).astype(jnp.int32), axis=1
            )
            for j in range(top)
        )
        target = jnp.tile(mine * cap + slot, FOLD)
        picks.append(
            (same_fold & (target[:, None] == (place // FOLD)[None, :])).astype(BF)
        )
    mixed, sent = mix(projected, residual, expert_norm_scale, sum(picks).T)
    blocks = (NZ * NC, cap * FOLD, depth // FOLD)
    arrived = exchange(sent.reshape(blocks), ("z", "c"))

    rows = exchange(deal(arrived.reshape(sent.shape)), TP)
    partial = experts(rows.reshape(-1, depth), pieces)
    back = exchange(partial.reshape(rows.shape), TP)
    returned = exchange(collect(back).reshape(blocks), ("z", "c"))
    return finish(mixed, returned.reshape(sent.shape), route_weights, picks)


def solution(mesh):
    fine = Mesh(
        mesh.devices.reshape(NZ, NC, NYH, NYL, NX), ("z", "c", "yh", "yl", "x")
    )
    sp, both = ("z", "c"), ("z", "c", "yh", "yl", "x")
    placed = (
        P(sp, TP),
        P(sp, None),
        P(sp, None),
        P(),
        P(),
        P(None, TP),
        P(),
        P(both, None),
        P(both, None),
        P(both, None),
        P(sp, None, TP),
        P(sp, None, TP),
        P(sp, TP, None),
    )
    return jax.shard_map(
        local, mesh=fine, in_specs=placed, out_specs=P(both, None), check_vma=False
    )
```

```python
import math

import jax
import jax.numpy as jnp
from jax import lax
from jax.experimental import pallas as pl
from jax.experimental.pallas import tpu as pltpu
from jax.sharding import Mesh, PartitionSpec as P


GRID_W = 64
EPS = 1e-06
ROPE_BASE = 10000.0
LOG2E = 1.4426950408889634
BF = jnp.bfloat16
F32 = jnp.float32

NZ, NC, NYH, NYL, NX = 16, 2, 2, 2, 4
NY = NYH * NYL
NT = NY * NX
NG = NYL * NX
TP = ("yh", "yl", "x")
GROUP = ("yl", "x")
STAT_ROWS = 16
FOLD = 8
EXPERT_GRANT = 46
SHARE = 128
NSHARE = 4
COLOURS = tuple((i % NX + i // NX) % NSHARE for i in range(NT))


IN_VMEM = pl.BlockSpec(memory_space=pltpu.VMEM)
IN_HBM = pl.BlockSpec(memory_space=pltpu.HBM)


def grant(mib):
    return pltpu.CompilerParams(vmem_limit_bytes=mib * 1024 * 1024)


def exchange(blocks, axis):
    return lax.all_to_all(blocks, axis, split_axis=0, concat_axis=0, tiled=True)


def swap_cores(value):
    return lax.ppermute(value, "c", [(0, 1), (1, 0)])


def ring(value, axis, step):
    return lax.ppermute(value, axis, [(i, (i + step) % 4) for i in range(4)])


def turned(field, gain, start):
    count, width = field.shape
    quarter = width // 4
    f = field.astype(F32)
    f = f * lax.rsqrt(jnp.mean(f * f, axis=-1, keepdims=True) + EPS) * gain
    lane = lax.broadcasted_iota(jnp.int32, (count, width), 1)
    position = start + lax.broadcasted_iota(jnp.int32, (count, width), 0)
    coord = jnp.where(lane < 2 * quarter, position // GRID_W, position % GRID_W)
    step = (lane % quarter).astype(F32) / quarter
    angle = coord.astype(F32) * jnp.exp(step * (-math.log(ROPE_BASE)))
    first = lane % (2 * quarter) < quarter
    ahead = pltpu.roll(f, width - quarter, 1)
    behind = pltpu.roll(f, quarter, 1)
    other = jnp.where(first, -ahead, behind)
    return (f * jnp.cos(angle) + other * jnp.sin(angle)).astype(BF)


def prepare_kernel(at_ref, q_ref, k_ref, v_ref, q_gain_ref, k_gain_ref, q8_ref, kv_ref):
    q_rot = turned(q_ref[...], q_gain_ref[...], at_ref[2])
    for i in range(q8_ref.shape[0]):
        q8_ref[i] = q_rot
    k_rot = turned(k_ref[...], k_gain_ref[...], at_ref[3])
    both = jnp.concatenate([k_rot, v_ref[...]], axis=1)
    for i in range(kv_ref.shape[0]):
        kv_ref[i] = both


def prepare(queries, keys, values, query_gain, key_gain, block, head, start):
    tokens, width = queries.shape
    size = tokens // NG
    at = jnp.stack([block, head, start, start + block * size]).astype(jnp.int32)
    whole = lambda shape: pl.BlockSpec(shape, lambda i, at: (0,) * len(shape))
    part = pl.BlockSpec((size, width), lambda i, at: (at[0], at[1]))
    outs = ((NG, tokens, width), (NZ, size, 2 * width))
    return pl.pallas_call(
        prepare_kernel,
        grid_spec=pltpu.PrefetchScalarGridSpec(
            num_scalar_prefetch=1,
            grid=(1,),
            in_specs=[whole((tokens, width)), part, part, whole((1, width)), whole((1, width))],
            out_specs=[whole(shape) for shape in outs],
        ),
        out_shape=[jax.ShapeDtypeStruct(shape, BF) for shape in outs],
        name="prepare",
    )(at, queries, keys, values, query_gain[None, :], key_gain[None, :])


def split3(x):
    hi = x.astype(BF)
    rest = x - hi.astype(F32)
    mid = rest.astype(BF)
    lo = (rest - mid.astype(F32)).astype(BF)
    return hi, mid, lo


def attend_kernel(q_ref, own_ref, other_ref, out_ref, scores_ref):
    heads, rows, width = q_ref.shape
    factor = width ** (-0.5) * LOG2E
    keys = jnp.concatenate([own_ref[:, :width], other_ref[:, :width]], axis=0)
    values = jnp.concatenate([own_ref[:, width:], other_ref[:, width:]], axis=0)
    values = jnp.concatenate(
        [values.T, jnp.ones((STAT_ROWS, values.shape[0]), BF)], axis=0
    )
    row = lax.broadcasted_iota(jnp.int32, (STAT_ROWS, rows), 0)

    def score(head):
        scores_ref[head % 2] = lax.dot_general(
            keys, q_ref[head], (((1,), (1,)), ((), ())), preferred_element_type=F32
        )

    score(0)
    for head in range(heads):
        if head + 1 < heads:
            score(head + 1)
        scores = scores_ref[head % 2]
        top = jnp.max(scores, axis=0, keepdims=True)
        weights = jnp.exp2((scores - top) * factor).astype(BF)
        summed = jnp.dot(values, weights, preferred_element_type=F32)
        total = summed[width : width + 1]
        out_ref[head, :width, :] = (summed[:width] * (1.0 / total)).astype(BF)
        stats = jnp.zeros((STAT_ROWS, rows), F32)
        for i, part in enumerate(split3(top * factor) + split3(total)):
            stats = jnp.where(row == i, part.astype(F32), stats)
        out_ref[head, width:, :] = stats.astype(BF)


def attend(q8, own, other):
    heads, rows, width = q8.shape
    return pl.pallas_call(
        attend_kernel,
        in_specs=[IN_VMEM] * 3,
        out_specs=IN_VMEM,
        out_shape=jax.ShapeDtypeStruct((heads, width + STAT_ROWS, rows), BF),
        scratch_shapes=[pltpu.VMEM((2, NC * own.shape[0], rows), F32)],
        compiler_params=grant(24),
        name="attend",
    )(q8, own, other)


def combine_kernel(parts_ref, out_ref):
    count = parts_ref.shape[0]
    width = out_ref.shape[1]
    tops, totals = [], []
    for j in range(count):
        s = parts_ref[j, width:, :].astype(F32)
        tops.append(s[0:1] + s[1:2] + s[2:3])
        totals.append(s[3:4] + s[4:5] + s[5:6])
    top = tops[0]
    for j in range(1, count):
        top = jnp.maximum(top, tops[j])
    shares = [totals[j] * jnp.exp2(tops[j] - top) for j in range(count)]
    whole = sum(shares[1:], shares[0])
    acc = jnp.zeros((width, parts_ref.shape[2]), F32)
    for j in range(count):
        acc = acc + parts_ref[j, :width, :].astype(F32) * (shares[j] / whole)
    done = acc.astype(BF)
    part = done.shape[1] // (NYH * NYL)
    halves = [
        jnp.concatenate(
            [
                done[:, (NYL * i + k) * part : (NYL * i + k + 1) * part]
                for i in range(NYH)
            ],
            axis=1,
        )
        for k in range(NYL)
    ]
    for i in range(out_ref.shape[0]):
        out_ref[i] = halves[i // NX % NYL]


def combine(parts):
    width = parts.shape[1] - STAT_ROWS
    return pl.pallas_call(
        combine_kernel,
        in_specs=[IN_VMEM],
        out_specs=IN_VMEM,
        out_shape=jax.ShapeDtypeStruct((NT, width, parts.shape[2] // NYL), BF),
        compiler_params=grant(16),
        name="combine",
    )(parts)


def folded(rows):
    width = rows.shape[1] // FOLD
    return jnp.concatenate(
        [rows[:, j * width : (j + 1) * width] for j in range(FOLD)], axis=0
    )


def picking(outs, ins, source_of):
    i = lax.broadcasted_iota(jnp.int32, (outs, ins), 0)
    r = lax.broadcasted_iota(jnp.int32, (outs, ins), 1)
    return jnp.where(r == source_of(i), 1.0, 0.0).astype(BF)


def mix_kernel(
    yl_ref, projected_ref, residual_ref, scale_ref, selector_ref, mixed_ref, sent_ref
):
    width = projected_ref.shape[2] // NYL
    projected = jnp.concatenate(
        [
            jnp.where(
                yl_ref[0] == k,
                projected_ref[NX * h + i, :, :width].astype(F32),
                projected_ref[NX * h + i, :, width:].astype(F32),
            )
            for h in range(NYH)
            for k in range(NYL)
            for i in range(NX)
        ],
        axis=1,
    )
    mixed = (residual_ref[...].astype(F32) + projected).astype(BF)
    mixed_ref[...] = mixed
    mixed = mixed.astype(F32)
    mean = jnp.mean(mixed * mixed, axis=-1, keepdims=True)
    normed = (mixed * lax.rsqrt(mean + EPS) * scale_ref[...]).astype(BF)
    sent_ref[...] = jnp.dot(
        selector_ref[...], folded(normed), preferred_element_type=F32
    ).astype(BF)


def mix(yl, projected, residual, scale, selector):
    shape = (selector.shape[0], residual.shape[1] // FOLD)
    return pl.pallas_call(
        mix_kernel,
        in_specs=[pl.BlockSpec(memory_space=pltpu.SMEM)] + [IN_VMEM] * 4,
        out_specs=[IN_VMEM] * 2,
        out_shape=[
            jax.ShapeDtypeStruct(residual.shape, BF),
            jax.ShapeDtypeStruct(shape, BF),
        ],
        compiler_params=grant(16),
        name="mix",
    )(yl.reshape(1).astype(jnp.int32), projected, residual, scale[None, :], selector)


def deal_kernel(arrived_ref, out_ref):
    total, _ = arrived_ref.shape
    count, each = total // FOLD, out_ref.shape[1]
    unfold = picking(total, total, lambda i: i % count * FOLD + i // count)
    rows = jnp.dot(unfold, arrived_ref[...], preferred_element_type=F32).astype(BF)
    for k in range(NSHARE):
        mine = jnp.concatenate(
            [rows[j * count + k * each : j * count + (k + 1) * each] for j in range(FOLD)],
            axis=1,
        )
        for i, colour in enumerate(COLOURS):
            if colour == k:
                out_ref[i] = mine


def deal(arrived):
    total, width = arrived.shape
    return pl.pallas_call(
        deal_kernel,
        in_specs=[IN_VMEM],
        out_specs=IN_VMEM,
        out_shape=jax.ShapeDtypeStruct((NT, total // FOLD // NSHARE, width * FOLD), BF),
        compiler_params=grant(16),
        name="deal",
    )(arrived)


def collect_kernel(back_ref, out_ref):
    classes = []
    for k in range(NSHARE):
        total = None
        for i, colour in enumerate(COLOURS):
            if colour == k:
                part = back_ref[i].astype(F32)
                total = part if total is None else total + part
        classes.append(total.astype(BF))
    rows = jnp.concatenate(classes, axis=0)
    count = rows.shape[0]
    fold = picking(
        FOLD * count, FOLD * count, lambda i: i % FOLD * count + i // FOLD
    )
    out_ref[...] = jnp.dot(fold, folded(rows), preferred_element_type=F32).astype(BF)


def collect(back):
    _, each, depth = back.shape
    return pl.pallas_call(
        collect_kernel,
        in_specs=[IN_VMEM],
        out_specs=IN_VMEM,
        out_shape=jax.ShapeDtypeStruct((NSHARE * each * FOLD, depth // FOLD), BF),
        compiler_params=grant(16),
        name="collect",
    )(back)


def finish_kernel(mixed_ref, returned_ref, weights_ref, *refs):
    picks, out_ref = refs[:-1], refs[-1]
    tokens, depth = mixed_ref.shape
    width = depth // FOLD
    found = [
        jnp.dot(pick[...], returned_ref[...], preferred_element_type=F32) for pick in picks
    ]
    for j in range(FOLD):
        cols, rows = slice(j * width, (j + 1) * width), slice(j * tokens, (j + 1) * tokens)
        moe = sum(f[rows] * weights_ref[:, k : k + 1] for k, f in enumerate(found))
        out_ref[:, cols] = (mixed_ref[:, cols].astype(F32) + moe).astype(BF)


def finish(mixed, returned, weights, picks):
    return pl.pallas_call(
        finish_kernel,
        in_specs=[IN_VMEM] * (3 + len(picks)),
        out_specs=IN_VMEM,
        out_shape=jax.ShapeDtypeStruct(mixed.shape, BF),
        compiler_params=grant(16),
        name="finish",
    )(mixed, returned, weights, *picks)


def pack_kernel(gate_ref, up_ref, down_ref, *out_refs):
    gate_up = jnp.concatenate([gate_ref[0].T, up_ref[0].T], axis=0)
    for half in range(2):
        @pl.when(pl.program_id(0) == half)
        def _():
            out_refs[half][...] = gate_up
            out_refs[2 + half][...] = down_ref[0]


def pack(w_gate, w_up, w_down):
    _, depth, units = w_gate.shape
    wide = pl.BlockSpec((1, depth, SHARE), lambda i: (0, 0, i))
    shapes = [(2 * SHARE, depth)] * 2 + [(SHARE, depth)] * 2
    outs = pl.pallas_call(
        pack_kernel,
        grid=(units // SHARE,),
        in_specs=[wide, wide, pl.BlockSpec((1, SHARE, depth), lambda i: (0, i, 0))],
        out_specs=[pl.BlockSpec(shape, lambda i: (0, 0)) for shape in shapes],
        out_shape=[jax.ShapeDtypeStruct(shape, BF) for shape in shapes],
        name="pack",
    )(w_gate, w_up, w_down)
    return outs[:2], outs[2:]


def experts_kernel(rows_ref, *refs):
    pieces, (out_ref, held, acc, sems) = refs[:-4], refs[-4:]
    pairs = len(pieces) // 4
    ups, downs = pieces[: 2 * pairs], pieces[2 * pairs :]
    copies = []
    for p in range(pairs):
        for j in range(3):
            for i in range(2):
                source = downs[2 * p + i]
                if j < 2:
                    source = ups[2 * p + i].at[pl.ds(j * SHARE, SHARE)]
                copies.append(
                    pltpu.make_async_copy(
                        source, held.at[p, j, pl.ds(i * SHARE, SHARE)], sems.at[p, j, i]
                    )
                )
    for copy in copies[:12]:
        copy.start()
    across = (((1,), (1,)), ((), ()))
    for p in range(pairs):
        gate_up = []
        for j in range(2):
            for copy in copies[6 * p + 2 * j : 6 * p + 2 * j + 2]:
                copy.wait()
            gate_up.append(
                lax.dot_general(
                    rows_ref[...], held[p, j], across, preferred_element_type=F32
                )
            )
        gate, upper = gate_up
        hidden = (gate / (1.0 + jnp.exp(-gate)) * upper).astype(BF)
        for copy in copies[6 * p + 4 : 6 * p + 6]:
            copy.wait()
        for copy in copies[6 * (p + 2) : 6 * (p + 3)]:
            copy.start()
        part = jnp.dot(hidden, held[p, 2], preferred_element_type=F32)
        if p == 0:
            acc[...] = part
        elif p < pairs - 1:
            acc[...] += part
        else:
            out_ref[...] = (acc[...] + part).astype(BF)


def experts(rows, pieces):
    pairs, depth = len(pieces) // 4, rows.shape[1]
    return pl.pallas_call(
        experts_kernel,
        in_specs=[IN_VMEM] + [IN_HBM] * len(pieces),
        out_specs=IN_VMEM,
        out_shape=jax.ShapeDtypeStruct(rows.shape, BF),
        scratch_shapes=[
            pltpu.VMEM((pairs, 3, 2 * SHARE, depth), BF),
            pltpu.VMEM(rows.shape, F32),
            pltpu.SemaphoreType.DMA((pairs, 3, 2)),
        ],
        compiler_params=grant(EXPERT_GRANT),
        name="experts",
    )(rows, *pieces)


def local(
    queries,
    keys,
    values,
    query_gain,
    key_gain,
    out_proj,
    expert_norm_scale,
    residual,
    routes,
    route_weights,
    w_gate,
    w_up,
    w_down,
):
    width = query_gain.shape[0]
    tok_sp = queries.shape[0]
    tok_dev, depth = residual.shape
    top = routes.shape[1]
    z, c = lax.axis_index("z"), lax.axis_index("c")
    yh, yl, x = lax.axis_index("yh"), lax.axis_index("yl"), lax.axis_index("x")
    start = (z * NC + c) * tok_sp

    q8, kv = prepare(
        queries, keys, values, query_gain, key_gain, yl * NX + x, yh, start
    )
    q8 = exchange(q8, GROUP)
    out_proj_other = lax.ppermute(out_proj, "yl", [(0, 1), (1, 0)])
    q8, kv = lax.optimization_barrier((q8, kv))
    kv_mine = exchange(kv, "z").reshape(-1, 2 * width)
    kv_other = swap_cores(kv_mine)

    ups, downs = pack(w_gate, w_up, w_down)
    axes = ("x", ("yh", "yl"))
    pieces = []
    for packs in (ups, downs):
        left = [ring(p, axis, 1) for p, axis in zip(packs, axes)]
        right = [ring(p, axis, -1) for p, axis in zip(packs, axes)]
        last = [ring(p, axis, 1) for p, axis in zip(left, axes)]
        pieces += [*packs, *left, *right, *last]

    parts = attend(q8, kv_mine, kv_other)
    parts = exchange(parts, GROUP)
    attn_all = exchange(combine(parts), TP).reshape(NT * width, -1)

    both_proj = jnp.concatenate([out_proj, out_proj_other], axis=1)
    columns = lax.dot_general(
        attn_all, both_proj, (((0,), (0,)), ((), ())), preferred_element_type=F32
    ).astype(BF)
    projected = exchange(columns.reshape(NYH * NX, tok_dev, -1), ("yh", "x"))

    cap = max(2, 2 * tok_dev * top // (NZ * NC))
    tok = jnp.arange(tok_dev, dtype=jnp.int32)
    before = tok[None, :] < tok[:, None]
    place = jnp.arange(NZ * NC * cap * FOLD, dtype=jnp.int32)
    row = jnp.arange(FOLD * tok_dev, dtype=jnp.int32)
    same_fold = (row // tok_dev)[:, None] == (place % FOLD)[None, :]
    picks = []
    for k in range(top):
        mine = routes[:, k]
        slot = sum(
            jnp.sum(
                ((mine[:, None] == routes[:, j][None, :]) & before).astype(jnp.int32), axis=1
            )
            for j in range(top)
        )
        target = jnp.tile(mine * cap + slot, FOLD)
        picks.append(
            (same_fold & (target[:, None] == (place // FOLD)[None, :])).astype(BF)
        )
    mixed, sent = mix(yl, projected, residual, expert_norm_scale, sum(picks).T)
    blocks = (NZ * NC, cap * FOLD, depth // FOLD)
    arrived = exchange(sent.reshape(blocks), ("z", "c"))

    rows = exchange(deal(arrived.reshape(sent.shape)), TP)
    partial = experts(rows.reshape(-1, depth), pieces)
    back = exchange(partial.reshape(rows.shape), TP)
    returned = exchange(collect(back).reshape(blocks), ("z", "c"))
    return finish(mixed, returned.reshape(sent.shape), route_weights, picks)


def solution(mesh):
    fine = Mesh(
        mesh.devices.reshape(NZ, NC, NYH, NYL, NX), ("z", "c", "yh", "yl", "x")
    )
    sp, both = ("z", "c"), ("z", "c", "yh", "yl", "x")
    placed = (
        P(sp, TP),
        P(sp, None),
        P(sp, None),
        P(),
        P(),
        P(None, TP),
        P(),
        P(both, None),
        P(both, None),
        P(both, None),
        P(sp, None, TP),
        P(sp, None, TP),
        P(sp, TP, None),
    )
    return jax.shard_map(
        local, mesh=fine, in_specs=placed, out_specs=P(both, None), check_vma=False
    )
```
